32 devices in a mesh: grp: 2 (over y), kv: 4 (over z), tp: 4 (over x, core).
Axes of the slice: x: 2, y: 2, z: 4, core: 2. Of those that a mesh axis runs over, the one named last changes fastest.
Arguments:
- tokens: bfloat16 [128, 2048], P('grp', 'kv'), parts along dimension 0, may hold values from -64 to 64
- lengths: int32 [128], P(('grp', 'kv')), parts along dimension 0, may hold values from 1 to 4096, 32768 in all
- state: float32 [128, 8, 128, 256], P(('grp', 'kv'), 'tp'), parts along dimension 0, may hold values from -6 to 6
- key_block: bfloat16 [128, 8, 64, 128], P(('grp', 'kv'), 'tp'), parts along dimension 0, may hold values from -6 to 6
- value_block: bfloat16 [128, 8, 64, 256], P(('grp', 'kv'), 'tp'), parts along dimension 0, may hold values from -6 to 6
- cum_decay: float32 [128, 8, 64, 128], P(('grp', 'kv'), 'tp'), parts along dimension 0, as said below
- step_decay: float32 [128, 1024], P(('grp', 'kv'), 'tp'), parts along dimension 0
- g_mix: bfloat16 [2048], P('kv'), may hold values from 0.099609375 to 1.8984375
- w_query: bfloat16 [2048, 1024], P('kv', 'tp'), may hold values from -0.125 to 0.125
- w_key: bfloat16 [2048, 1024], P('kv', 'tp'), may hold values from -0.125 to 0.125
- w_value: bfloat16 [2048, 2048], P('kv', 'tp'), may hold values from -0.125 to 0.125
- w_outgate: bfloat16 [2048, 2048], P('kv', 'tp'), may hold values from -0.125 to 0.125
- w_decay: bfloat16 [2048, 1024], P('kv', 'tp'), may hold values from -0.5 to 0.5
- g_heads: bfloat16 [2048], P('tp'), may hold values from 0.099609375 to 1.8984375
- w_out: bfloat16 [2048, 2048], P('tp', 'kv'), may hold values from -0.125 to 0.125
- g_ffn: bfloat16 [2048], P('kv'), may hold values from 0.099609375 to 1.8984375
- w_gate: bfloat16 [2048, 5632], P('kv', 'tp'), may hold values from -0.125 to 0.125
- w_up: bfloat16 [2048, 5632], P('kv', 'tp'), may hold values from -0.125 to 0.125
- w_down: bfloat16 [5632, 2048], P('tp', 'kv'), may hold values from -0.078125 to 0.078125
Outputs:
- updated: bfloat16 [128, 2048], P('grp', 'kv'), parts along dimension 0
The draws below stay inside these ranges and needn't reach their ends.
There are 2 independent parts, one for each index of `grp`. The reference program is written for one: setup_inputs(seed, part) draws one part's arguments, and reference() takes and returns one part's arrays. A program takes and returns all parts, laid end to end along the dimension named above; an argument that names none is the same for every part. Nothing has to cross between parts.
Inputs may be any that keep to these rules, and one draw needn't show every extreme that they name: `cum_decay`: along the block's positions the entries never rise.
All inputs are finite; a program needn't handle non-finite values. No bound on the sum of `lengths` on one device may be relied on, other than what follows from the above.
Results may differ from the reference program's by a relative error of at most 0.019.
Values may be sent and summed in bfloat16 or wider, within the bound.
A program may use at most 64 MiB of HBM per device.

```python
import math
import jax
import jax.numpy as jnp
import numpy as np
from jax import lax

D = 2048
ATTN_GROUPS = 8
DK = 128
DV = 256
FF = 5632
SPAN_STEPS = 64
STREAM_NUMBER = 64
N_TP = 4


def head_rates(key):
    k_slow, k_fast, k_seq, k_chan = jax.random.split(key, 4)
    gradual_shrink_factor = jax.random.bernoulli(k_slow, 0.5, (1, ATTN_GROUPS, 1))
    fast_rate = jax.random.uniform(k_fast, (1, ATTN_GROUPS, 1), jnp.float32, 1.0 / 50.0, 1.0 / 30.0)
    slow_rate = jnp.float32(0.5 / SPAN_STEPS)
    seq_factor = jnp.exp(jax.random.uniform(k_seq, (STREAM_NUMBER, 1, 1), jnp.float32, math.log(0.5), math.log(2.0)))
    chan_factor = jax.random.uniform(k_chan, (1, ATTN_GROUPS, DK), jnp.float32, 0.5, 1.5)
    rate = jnp.where(gradual_shrink_factor, slow_rate, fast_rate) * seq_factor * chan_factor
    return (rate, gradual_shrink_factor)


def draw_tokens(key, part):
    k_base, k_rise, k_rows = jax.random.split(key, 3)
    columns = jnp.arange(D, dtype=jnp.float32) / D
    rough = jax.random.uniform(k_rise, (D,), jnp.float32, 0.5, 2.0)
    rows = jnp.exp(jax.random.uniform(k_rows, (STREAM_NUMBER, 1), jnp.float32, math.log(0.3), math.log(3.0)))
    base = jnp.clip(jax.random.normal(k_base, (STREAM_NUMBER, D), jnp.float32), -6.0, 6.0)
    rise = 3.0 ** columns * rough / 1.8
    return (base * rise[None, :] * rows).astype(jnp.bfloat16)


def draw_cum_decay(key, part):
    rate, gradual_shrink_factor = head_rates(jax.random.fold_in(key, 11))
    k_step, lookup_location, lookup_breadth = jax.random.split(jax.random.fold_in(key, 12), 3)
    steps = -rate[:, :, None, :] * jax.random.uniform(k_step, (STREAM_NUMBER, ATTN_GROUPS, SPAN_STEPS, DK), jnp.float32, 0.5, 1.5)
    span_offset = jax.random.randint(lookup_location, (STREAM_NUMBER, ATTN_GROUPS, 1, 2), 0, SPAN_STEPS)
    token_ordinal = jnp.arange(SPAN_STEPS, dtype=jnp.int32)[None, None, :, None]
    match_tally = jnp.any(token_ordinal == span_offset, axis=3)
    span_extent = jnp.log(jax.random.uniform(lookup_breadth, (STREAM_NUMBER, ATTN_GROUPS, 1), jnp.float32, 0.5, 0.8))
    surplus_tally = jnp.where(match_tally & gradual_shrink_factor, span_extent, jnp.float32(0.0))
    steps = steps + surplus_tally[:, :, :, None]
    return jnp.cumsum(steps, axis=2).astype(jnp.float32)


def draw_step_decay(key, part):
    rate, gradual_shrink_factor = head_rates(jax.random.fold_in(key, 11))
    k_step, lookup_location, lookup_breadth = jax.random.split(jax.random.fold_in(key, 13), 3)
    k_rough = jax.random.fold_in(key, 14)
    payload_element = -rate * jax.random.uniform(k_step, (STREAM_NUMBER, ATTN_GROUPS, DK), jnp.float32, 0.5, 1.5)
    payload_element = payload_element - jax.random.uniform(k_rough, (STREAM_NUMBER, ATTN_GROUPS, DK), jnp.float32, 0.0, 0.35)
    match_tally = jax.random.randint(lookup_location, (STREAM_NUMBER, ATTN_GROUPS, 1), 0, 2) == 0
    span_extent = jnp.log(jax.random.uniform(lookup_breadth, (STREAM_NUMBER, ATTN_GROUPS, 1), jnp.float32, 0.5, 0.8))
    payload_element = payload_element + jnp.where(match_tally & gradual_shrink_factor, span_extent, jnp.float32(0.0))
    return payload_element.reshape(STREAM_NUMBER, ATTN_GROUPS * DK).astype(jnp.float32)


def shard_levels(own_key, dims, shards, low, largest):
    level, own = 1.0, jax.random.fold_in(own_key, 6)
    for position, shards_of in shards:
        heights = jnp.exp(jax.random.uniform(jax.random.fold_in(own, position), (shards_of,), jnp.float32, low / len(shards), largest / len(shards)))
        level = level * jnp.repeat(heights, dims[position] // shards_of).reshape([-1 if axis == position else 1 for axis in range(len(dims))])
    return level


def length_profile(count, total, limit, skew):
    weights = [(1 << 20) // math.isqrt(grade ** skew) + 1 for grade in range(2, count + 1)]
    rest, given = total - limit - (count - 1), [1] * (count - 1)
    while rest > 0:
        movable = [i for i in range(count - 1) if given[i] < limit]
        mass, left = sum([weights[i] for i in movable]), rest
        for i in movable:
            extra = min(limit - given[i], max(1, left * weights[i] // mass), rest)
            given[i] = given[i] + extra
            rest = rest - extra
    return np.array([limit] + given)


def uneven_parts(own_key, amount, total, limit, lean):
    if amount == 2:
        one = jax.random.randint(own_key, (), max(1, total - limit), min(limit, total - 1) + 1)
        return jnp.stack([one, total - one])
    sizes = jnp.asarray(length_profile(amount, total, limit, lean), jnp.int32)
    twos = (amount - 1) // 2
    source_of, receiver = sizes[1:1 + 2 * twos:2], sizes[2:2 + 2 * twos:2]
    slack = jnp.minimum(source_of - 1, limit - receiver)
    moved = jax.random.randint(jax.random.fold_in(own_key, 1), (twos,), 0, 1 << 20) % (slack + 1)
    sizes = sizes.at[1:1 + 2 * twos:2].set(source_of - moved).at[2:2 + 2 * twos:2].set(receiver + moved)
    return sizes[jax.random.permutation(jax.random.fold_in(own_key, 2), amount)]


def gaussian(key, extent, scale, most, cuts=(), kind=jnp.bfloat16):
    factor_of = shard_levels(key, extent, cuts, -0.22, 0.18) if cuts else 1.0
    entries = jax.random.normal(key, extent, jnp.float32) * scale * factor_of
    return jnp.minimum(jnp.maximum(entries, -most), most).astype(kind)


def setup_inputs(seed: int = 0, part: int = 0) -> dict:
    streams_of = jax.random.split(jax.random.key(seed), 20)
    part_splits = jax.random.split(jax.random.fold_in(streams_of[19], part), 20)
    return {
        "tokens": draw_tokens(jax.random.fold_in(jax.random.fold_in(streams_of[19], part), 71), part),
        "lengths": uneven_parts(part_splits[1], STREAM_NUMBER, STREAM_NUMBER * 512, min(4096, STREAM_NUMBER * 256), 2).astype(jnp.int32),
        "state": gaussian(part_splits[2], (STREAM_NUMBER, ATTN_GROUPS, DK, DV), 1.0, 6.0, ((0, 4), (1, 4)), jnp.float32),
        "key_block": gaussian(part_splits[3], (STREAM_NUMBER, ATTN_GROUPS, SPAN_STEPS, DK), 1.0, 6.0, ((0, 4), (1, 4))),
        "value_block": gaussian(part_splits[4], (STREAM_NUMBER, ATTN_GROUPS, SPAN_STEPS, DV), 1.0, 6.0, ((0, 4), (1, 4))),
        "cum_decay": draw_cum_decay(jax.random.fold_in(jax.random.fold_in(streams_of[19], part), 71), part),
        "step_decay": draw_step_decay(jax.random.fold_in(jax.random.fold_in(streams_of[19], part), 71), part),
        "g_mix": jnp.clip(1.0 + 0.18 * jax.random.normal(streams_of[7], (D,), jnp.float32), 0.099609375, 1.8984375).astype(jnp.bfloat16),
        "w_query": gaussian(streams_of[8], (D, ATTN_GROUPS * DK), D ** -0.5, 0.125, ((0, 4), (1, 4))),
        "w_key": gaussian(streams_of[9], (D, ATTN_GROUPS * DK), D ** -0.5, 0.125, ((0, 4), (1, 4))),
        "w_value": gaussian(streams_of[10], (D, ATTN_GROUPS * DV), D ** -0.5, 0.125, ((0, 4), (1, 4))),
        "w_outgate": gaussian(streams_of[11], (D, ATTN_GROUPS * DV), D ** -0.5, 0.125, ((0, 4), (1, 4))),
        "w_decay": gaussian(streams_of[12], (D, ATTN_GROUPS * DK), (D // 16) ** -0.5, 0.5, ((0, 4), (1, 4))),
        "g_heads": jnp.clip(1.0 + 0.18 * jax.random.normal(streams_of[13], (ATTN_GROUPS * DV,), jnp.float32), 0.099609375, 1.8984375).astype(jnp.bfloat16),
        "w_out": gaussian(streams_of[14], (ATTN_GROUPS * DV, D), (ATTN_GROUPS * DV) ** -0.5, 0.125, ((0, 4), (1, 4))),
        "g_ffn": jnp.clip(1.0 + 0.18 * jax.random.normal(streams_of[15], (D,), jnp.float32), 0.099609375, 1.8984375).astype(jnp.bfloat16),
        "w_gate": gaussian(streams_of[16], (D, FF), D ** -0.5, 0.125, ((0, 4), (1, 4))),
        "w_up": gaussian(streams_of[17], (D, FF), D ** -0.5, 0.125, ((0, 4), (1, 4))),
        "w_down": gaussian(streams_of[18], (FF, D), FF ** -0.5, 0.078125, ((0, 4), (1, 4))),
    }


epsilon = 1e-06
temper = 16.0

def blocked_product(left, weight):
    block_rows = left.shape[1] // N_TP
    total = jnp.zeros((left.shape[0], weight.shape[1]), jnp.float32)
    for index in range(N_TP):
        part = jnp.dot(left[:, index * block_rows:(index + 1) * block_rows], weight[index * block_rows:(index + 1) * block_rows], preferred_element_type=jnp.float32)
        rounded = lax.optimization_barrier(part.astype(jnp.bfloat16))
        total = total + rounded.astype(jnp.float32)
    return total

def reference(tokens, lengths, state, key_block, value_block, cum_decay, step_decay, g_mix, w_query, w_key, w_value, w_outgate, w_decay, g_heads, w_out, g_ffn, w_gate, w_up, w_down):
    highest = lax.Precision.HIGHEST
    inputs = tokens.astype(jnp.float32)
    inverse = lax.rsqrt(lax.optimization_barrier(jnp.sum(inputs * inputs, axis=1)) / D + epsilon)[:, None]
    scaled = (inputs * g_mix.astype(jnp.float32)).astype(jnp.bfloat16)

    def project(matrix):
        return jnp.dot(scaled, matrix, preferred_element_type=jnp.float32) * inverse
    query = (project(w_query) * DK ** (-0.5)).reshape(STREAM_NUMBER, ATTN_GROUPS, DK)
    keys_new = project(w_key).reshape(STREAM_NUMBER, ATTN_GROUPS, DK)
    values_new = project(w_value).reshape(STREAM_NUMBER, ATTN_GROUPS, DV)
    out_gate = project(w_outgate)
    decay_pre = project(w_decay)
    log_step = (jax.nn.log_sigmoid(decay_pre) / temper + step_decay).reshape(STREAM_NUMBER, ATTN_GROUPS, DK)
    live_count = lengths % SPAN_STEPS
    token_ordinal = lax.broadcasted_iota(jnp.int32, (1, 1, SPAN_STEPS, 1), 2)
    picked = jnp.where(token_ordinal == live_count[:, None, None, None] - 1, cum_decay, jnp.float32(0.0))
    token_decay = lax.optimization_barrier(jnp.sum(picked, axis=2)) + log_step
    carried = jnp.einsum('shk,shkv->shv', query * jnp.exp(token_decay), state, precision=highest)
    scores = lax.optimization_barrier(jnp.sum(query[:, :, None, :] * key_block.astype(jnp.float32) * jnp.exp(token_decay[:, :, None, :] - cum_decay), axis=3))
    scores = jnp.where(token_ordinal[..., 0] < live_count[:, None, None], scores, jnp.float32(0.0))
    in_block = jnp.einsum('shj,shjv->shv', scores, value_block.astype(jnp.float32), precision=highest)
    own_term = lax.optimization_barrier(jnp.sum(query * keys_new, axis=2))[:, :, None] * values_new
    head_out = carried + in_block + own_term
    normed = head_out * lax.rsqrt(lax.optimization_barrier(jnp.mean(head_out * head_out, axis=2, keepdims=True)) + epsilon)
    normed = normed * g_heads.astype(jnp.float32).reshape(ATTN_GROUPS, DV)
    mixed = (normed.reshape(STREAM_NUMBER, ATTN_GROUPS * DV) * jax.nn.silu(out_gate)).astype(jnp.bfloat16)
    attention = blocked_product(mixed, w_out)
    residual = (inputs + attention).astype(jnp.bfloat16)
    middle = residual.astype(jnp.float32)
    mid_inverse = lax.rsqrt(lax.optimization_barrier(jnp.sum(middle * middle, axis=1)) / D + epsilon)[:, None]
    normed_mid = (middle * g_ffn.astype(jnp.float32)).astype(jnp.bfloat16)
    gate_sum = jnp.dot(normed_mid, w_gate, preferred_element_type=jnp.float32) * mid_inverse
    up_sum = jnp.dot(normed_mid, w_up, preferred_element_type=jnp.float32) * mid_inverse
    hidden = (jax.nn.silu(gate_sum) * up_sum).astype(jnp.bfloat16)
    return (middle + blocked_product(hidden, w_down)).astype(jnp.bfloat16)
```

```python
import functools

import jax
import jax.numpy as jnp
from jax import lax
from jax.experimental import pallas as pl
from jax.experimental.pallas import tpu as pltpu
from jax.sharding import PartitionSpec as P

f32 = jnp.float32
bf16 = jnp.bfloat16
epsilon = 1e-06
temper = 16.0
LANES = 128
MESH = pl.DeviceIdType.MESH


def silu(v):
    return v / (1.0 + jnp.exp(-v))


def far_first(n):
    return sorted(range(1, n), key=lambda o: (-min(o, n - o), -o))


def split_hi_lo(total):
    lane = lax.broadcasted_iota(jnp.int32, (total.shape[0], LANES), 1)
    wide = jnp.broadcast_to(total, (total.shape[0], LANES))
    high = wide.astype(bf16).astype(f32)
    return jnp.where(lane < LANES // 2, high, wide - high).astype(bf16)


def join_hi_lo(block):
    return block[:, :1] + block[:, LANES // 2 : LANES // 2 + 1]


def kernel(
    cfg,
    lengths,
    *refs,
):
    (n_kv, n_tp, names, bounds) = cfg
    count = len(names)
    hbm = dict(zip(names, refs[:count]))
    out_hbm = refs[count]
    rest = refs[count + 1 :]
    vm = dict(zip(names, rest[:count]))
    (
        out_vm,
        td_base,
        state_bf,
        q_ref,
        td_ref,
        qe_ref,
        head_ref,
        a_send,
        a_recv,
        b_send,
        b_recv,
        mixed_all,
        attn_all,
        gu_send,
        gu_recv,
        hid_all,
        down_all,
        local_sem,
        send_sem,
        recv_sem,
    ) = rest[count:]

    kv = lax.axis_index("kv")
    tp = lax.axis_index("tp")
    seqs, heads, dk, dv = vm["state"].shape
    block_len = vm["key_block"].shape[2]
    rows = vm["tokens"].shape[0]
    width = vm["tokens"].shape[1] * n_kv
    kw = heads * dk
    vw = heads * dv

    copies = {}
    for index, name in enumerate(names):
        copies[name] = pltpu.make_async_copy(hbm[name], vm[name], local_sem.at[index])
    for name in names[:EARLY]:
        copies[name].start()

    barrier = pltpu.get_barrier_semaphore()
    for o in range(1, n_kv):
        pl.semaphore_signal(
            barrier, inc=1, device_id={"kv": lax.rem(kv + o, n_kv)}, device_id_type=MESH
        )
    for o in range(1, n_tp):
        pl.semaphore_signal(
            barrier, inc=1, device_id={"tp": lax.rem(tp + o, n_tp)}, device_id_type=MESH
        )

    def gain(name):
        return vm[name][...].astype(f32).reshape(1, -1)

    sem_next = [0]

    def remote(src, dst, axis, target):
        index = sem_next[0]
        sem_next[0] += 1
        copy = pltpu.make_async_remote_copy(
            src_ref=src,
            dst_ref=dst,
            send_sem=send_sem.at[index],
            recv_sem=recv_sem.at[index],
            device_id={axis: target},
            device_id_type=MESH,
        )
        copy.start()
        return copy

    def scatter(send, recv):
        result = []
        for o in far_first(n_kv):
            target = lax.rem(kv + o, n_kv)
            result.append(remote(send.at[target], recv.at[o - 1], "kv", target))
        return result

    def gather(buffer, axis):
        me, n = (kv, n_kv) if axis == "kv" else (tp, n_tp)
        return [
            remote(buffer.at[me], buffer.at[me], axis, lax.rem(me + o, n)) for o in far_first(n)
        ]

    def wait_all(started):
        for copy in started:
            copy.wait()

    def store_rows(buffer, lo, value):
        for d in range(n_kv):
            buffer[d, :, lo : lo + value.shape[1]] = value[d * seqs : (d + 1) * seqs]

    def reduced(send, recv, lo, hi):
        total = send[kv, :, lo:hi].astype(f32)
        for o in range(n_kv - 1):
            total = total + recv[o, :, lo:hi].astype(f32)
        return total

    copies["tokens"].wait()
    copies["g_mix"].wait()
    inputs = vm["tokens"][...].astype(f32)
    scaled = (inputs * gain("g_mix")).astype(bf16)
    store_rows(a_send, 3 * kw, split_hi_lo(jnp.sum(inputs * inputs, axis=1, keepdims=True)))
    for index, name in enumerate(("w_query", "w_key", "w_decay")):
        copies[name].wait()
        part = jnp.dot(scaled, vm[name][...], preferred_element_type=f32)
        store_rows(a_send, index * kw, part.astype(bf16))
    for name in names[EARLY:]:
        copies[name].start()
    pl.semaphore_wait(barrier, n_kv - 1 + n_tp - 1)
    sent_a = scatter(a_send, a_recv)
    for index, name in enumerate(("w_value", "w_outgate")):
        copies[name].wait()
        part = jnp.dot(scaled, vm[name][...], preferred_element_type=f32)
        store_rows(b_send, index * vw, part.astype(bf16))
    sent_b = scatter(b_send, b_recv)

    copies["cum_decay"].wait()
    copies["state"].wait()
    ordinal = lax.broadcasted_iota(jnp.int32, (block_len, dk), 0)

    group = 8 if seqs % 8 == 0 else seqs

    def prepare(step, carry):
        base = pl.multiple_of(step * group, group)
        for h in range(heads):
            ends = []
            for sub in range(group):
                s = base + sub
                live = lax.rem(lengths[s], block_len)
                picked = jnp.where(ordinal == live - 1, vm["cum_decay"][s, h], 0.0)
                ends.append(jnp.sum(picked, axis=0, keepdims=True))
                state_bf[s, h] = vm["state"][s, h].astype(bf16)
            td_base[pl.ds(base, group), h * dk : (h + 1) * dk] = jnp.concatenate(ends, axis=0)
        return carry

    lax.fori_loop(0, seqs // group, prepare, 0)
    for name in ("step_decay", "key_block", "value_block", "g_heads"):
        copies[name].wait()

    wait_all(sent_a)
    inverse = lax.rsqrt(
        join_hi_lo(reduced(a_send, a_recv, 3 * kw, 3 * kw + LANES)) / width + epsilon
    )
    query = reduced(a_send, a_recv, 0, kw) * inverse * dk ** (-0.5)
    keys_new = reduced(a_send, a_recv, kw, 2 * kw) * inverse
    decay_pre = reduced(a_send, a_recv, 2 * kw, 3 * kw) * inverse
    log_sigmoid = jnp.minimum(decay_pre, 0.0) - jnp.log(1.0 + jnp.exp(-jnp.abs(decay_pre)))
    log_step = log_sigmoid / temper + vm["step_decay"][...]
    token_decay = td_base[...] + log_step
    q_ref[...] = query
    td_ref[...] = token_decay
    qe_ref[...] = query * jnp.exp(token_decay)

    live_ordinal = lax.broadcasted_iota(jnp.int32, (block_len, 1), 0)

    def attend(step, carry):
        base = pl.multiple_of(step * group, group)
        for h in range(heads):
            cols = slice(h * dk, (h + 1) * dk)
            qs = q_ref[pl.ds(base, group), cols]
            tds = td_ref[pl.ds(base, group), cols]
            qes = qe_ref[pl.ds(base, group), cols]
            outs = []
            for sub in range(group):
                s = base + sub
                live = lax.rem(lengths[s], block_len)
                left = jnp.broadcast_to(qes[sub : sub + 1], (16, dk)).astype(bf16)
                carried = jnp.dot(left, state_bf[s, h], preferred_element_type=f32)[:1]
                scores = jnp.sum(
                    qs[sub : sub + 1]
                    * vm["key_block"][s, h].astype(f32)
                    * jnp.exp(tds[sub : sub + 1] - vm["cum_decay"][s, h]),
                    axis=1,
                    keepdims=True,
                )
                scores = jnp.where(live_ordinal < live, scores, 0.0)
                in_block = jnp.sum(
                    scores * vm["value_block"][s, h].astype(f32), axis=0, keepdims=True
                )
                outs.append(carried + in_block)
            head_ref[pl.ds(base, group), h * dv : (h + 1) * dv] = jnp.concatenate(outs, axis=0)
        return carry

    lax.fori_loop(0, seqs // group, attend, 0)

    wait_all(sent_b)
    for h in range(heads):
        cols = slice(h * dv, (h + 1) * dv)
        keys = slice(h * dk, (h + 1) * dk)
        values_new = reduced(b_send, b_recv, h * dv, (h + 1) * dv) * inverse
        out_gate = reduced(b_send, b_recv, vw + h * dv, vw + (h + 1) * dv) * inverse
        own = jnp.sum(query[:, keys] * keys_new[:, keys], axis=1, keepdims=True)
        head_out = head_ref[:, cols] + own * values_new
        scale = lax.rsqrt(jnp.mean(head_out * head_out, axis=1, keepdims=True) + epsilon)
        normed = head_out * scale * gain("g_heads")[:, cols]
        mixed_all[kv, :, cols] = (normed * silu(out_gate)).astype(bf16)
    sent = gather(mixed_all, "kv")
    copies["w_out"].wait()
    wait_all(sent)

    mixed = mixed_all[...].reshape(rows, vw)
    attn_all[tp] = jnp.dot(mixed, vm["w_out"][...], preferred_element_type=f32).astype(bf16)
    sent = gather(attn_all, "tp")
    copies["g_ffn"].wait()
    copies["w_gate"].wait()
    copies["w_up"].wait()
    wait_all(sent)
    attention = attn_all[0].astype(f32)
    for t in range(1, n_tp):
        attention = attention + attn_all[t].astype(f32)
    middle = (inputs + attention).astype(bf16).astype(f32)
    normed_mid = (middle * gain("g_ffn")).astype(bf16)

    sent_gu = []
    for c, (lo, hi) in enumerate(bounds):
        if c == 0:
            square = jnp.sum(middle * middle, axis=1, keepdims=True)
            store_rows(gu_send[c], 2 * (hi - lo), split_hi_lo(square))
        for index, name in enumerate(("w_gate", "w_up")):
            part = jnp.dot(normed_mid, vm[name][:, lo:hi], preferred_element_type=f32)
            store_rows(gu_send[c], index * (hi - lo), part.astype(bf16))
        sent_gu.append(scatter(gu_send[c], gu_recv[c]))
    sent_hid = []
    mid_inverse = None
    for c, (lo, hi) in enumerate(bounds):
        w = hi - lo
        wait_all(sent_gu[c])
        if c == 0:
            total = join_hi_lo(reduced(gu_send[c], gu_recv[c], 2 * w, 2 * w + LANES))
            mid_inverse = lax.rsqrt(total / width + epsilon)
        gate = reduced(gu_send[c], gu_recv[c], 0, w) * mid_inverse
        up = reduced(gu_send[c], gu_recv[c], w, 2 * w) * mid_inverse
        hid_all[c][kv] = (silu(gate) * up).astype(bf16)
        sent_hid.append(gather(hid_all[c], "kv"))
    copies["w_down"].wait()
    down = None
    for c, (lo, hi) in enumerate(bounds):
        wait_all(sent_hid[c])
        hidden = hid_all[c][...].reshape(rows, hi - lo)
        part = jnp.dot(hidden, vm["w_down"][lo:hi], preferred_element_type=f32)
        down = part if down is None else down + part
    down_all[tp] = down.astype(bf16)
    wait_all(gather(down_all, "tp"))
    total = down_all[0].astype(f32)
    for t in range(1, n_tp):
        total = total + down_all[t].astype(f32)
    out_hbm[...] = (middle + total).astype(bf16)


ORDER = (
    "tokens",
    "g_mix",
    "w_query",
    "w_key",
    "w_decay",
    "w_value",
    "w_outgate",
    "cum_decay",
    "state",
    "step_decay",
    "key_block",
    "value_block",
    "g_heads",
    "w_out",
    "g_ffn",
    "w_gate",
    "w_up",
    "w_down",
)
CHUNKS = 2
EARLY = 7


def body(n_kv, n_tp, lengths, given):
    rows, columns = given["tokens"].shape
    seqs, heads, dk, dv = given["state"].shape
    kw, vw = heads * dk, heads * dv
    hidden = given["w_gate"].shape[1]
    tiles = -(-hidden // LANES)
    chunks = min(CHUNKS, tiles)
    edges = [min(-(-tiles * c // chunks) * LANES, hidden) for c in range(chunks + 1)]
    bounds = tuple(zip(edges[:-1], edges[1:]))
    widths = [hi - lo for lo, hi in bounds]
    gu_widths = [2 * w + (LANES if c == 0 else 0) for c, w in enumerate(widths)]
    out_cols = given["w_out"].shape[1]
    remote_count = (n_kv - 1) * (3 + 2 * chunks) + 2 * (n_tp - 1)
    scratch = [pltpu.VMEM(given[name].shape, given[name].dtype) for name in ORDER]
    scratch += [
        pltpu.VMEM((rows, columns), bf16),
        pltpu.VMEM((seqs, kw), f32),
        pltpu.VMEM((seqs, heads, dk, dv), bf16),
        pltpu.VMEM((seqs, kw), f32),
        pltpu.VMEM((seqs, kw), f32),
        pltpu.VMEM((seqs, kw), f32),
        pltpu.VMEM((seqs, vw), f32),
        pltpu.VMEM((n_kv, seqs, 3 * kw + LANES), bf16),
        pltpu.VMEM((n_kv - 1, seqs, 3 * kw + LANES), bf16),
        pltpu.VMEM((n_kv, seqs, 2 * vw), bf16),
        pltpu.VMEM((n_kv - 1, seqs, 2 * vw), bf16),
        pltpu.VMEM((n_kv, seqs, vw), bf16),
        pltpu.VMEM((n_tp, rows, out_cols), bf16),
        [pltpu.VMEM((n_kv, seqs, w), bf16) for w in gu_widths],
        [pltpu.VMEM((n_kv - 1, seqs, w), bf16) for w in gu_widths],
        [pltpu.VMEM((n_kv, seqs, w), bf16) for w in widths],
        pltpu.VMEM((n_tp, rows, out_cols), bf16),
        pltpu.SemaphoreType.DMA((len(ORDER) + 1,)),
        pltpu.SemaphoreType.DMA((remote_count,)),
        pltpu.SemaphoreType.DMA((remote_count,)),
    ]
    cfg = (n_kv, n_tp, ORDER, bounds)
    return pl.pallas_call(
        functools.partial(kernel, cfg),
        out_shape=pltpu.VMEM((rows, columns), bf16),
        in_specs=[pl.BlockSpec(memory_space=pltpu.SMEM)]
        + [pl.BlockSpec(memory_space=pltpu.HBM)] * len(ORDER),
        out_specs=pl.BlockSpec(memory_space=pltpu.VMEM),
        scratch_shapes=scratch,
        compiler_params=pltpu.CompilerParams(collective_id=0, has_side_effects=True),
        name="layer",
    )(lengths, *[given[name] for name in ORDER])


NAMES = (
    "tokens",
    "lengths",
    "state",
    "key_block",
    "value_block",
    "cum_decay",
    "step_decay",
    "g_mix",
    "w_query",
    "w_key",
    "w_value",
    "w_outgate",
    "w_decay",
    "g_heads",
    "w_out",
    "g_ffn",
    "w_gate",
    "w_up",
    "w_down",
)


def solution(mesh):
    def call(*arrays):
        given = dict(zip(NAMES, arrays))
        lengths = given.pop("lengths")
        return body(mesh.shape["kv"], mesh.shape["tp"], lengths, given)

    return jax.shard_map(
        call,
        mesh=mesh,
        in_specs=(
            P("grp", "kv"),
            P(("grp", "kv")),
            P(("grp", "kv"), "tp", None, None),
            P(("grp", "kv"), "tp", None, None),
            P(("grp", "kv"), "tp", None, None),
            P(("grp", "kv"), "tp", None, None),
            P(("grp", "kv"), "tp"),
            P("kv"),
            P("kv", "tp"),
            P("kv", "tp"),
            P("kv", "tp"),
            P("kv", "tp"),
            P("kv", "tp"),
            P("tp"),
            P("tp", "kv"),
            P("kv"),
            P("kv", "tp"),
            P("kv", "tp"),
            P("tp", "kv"),
        ),
        out_specs=P("grp", "kv"),
        check_vma=False,
    )
```

```python
import functools

import jax
import jax.numpy as jnp
from jax import lax
from jax.experimental import pallas as pl
from jax.experimental.pallas import tpu as pltpu
from jax.sharding import PartitionSpec as P

f32 = jnp.float32
bf16 = jnp.bfloat16
epsilon = 1e-06
temper = 16.0
LANES = 128
MESH = pl.DeviceIdType.MESH


def silu(v):
    return v / (1.0 + jnp.exp(-v))


def far_first(n):
    return sorted(range(1, n), key=lambda o: (-min(o, n - o), -o))


def split_hi_lo(total):
    lane = lax.broadcasted_iota(jnp.int32, (total.shape[0], LANES), 1)
    wide = jnp.broadcast_to(total, (total.shape[0], LANES))
    high = wide.astype(bf16).astype(f32)
    return jnp.where(lane < LANES // 2, high, wide - high).astype(bf16)


def join_hi_lo(block):
    return block[:, :1] + block[:, LANES // 2 : LANES // 2 + 1]


def kernel(
    cfg,
    lengths,
    *refs,
):
    (n_kv, n_tp, names, bounds, parts) = cfg
    count = len(names)
    hbm = dict(zip(names, refs[:count]))
    out_ref = refs[count]
    rest = refs[count + 1 :]
    vm = dict(zip(names, rest[:count]))
    (
        td_base,
        state_bf,
        q_ref,
        td_ref,
        qe_ref,
        head_ref,
        a_send,
        a_recv,
        b_send,
        b_recv,
        a_merge,
        b_merge,
        mixed_all,
        attn_all,
        gu_send,
        gu_recv,
        gu_merge,
        hid_all,
        down_all,
        local_sem,
        send_sem,
        recv_sem,
    ) = rest[count:]

    kv = lax.axis_index("kv")
    tp = lax.axis_index("tp")
    seqs, heads, dk, dv = vm["state"].shape
    block_len = vm["key_block"].shape[2]
    width = vm["tokens"].shape[1] * n_kv
    kw = heads * dk
    vw = heads * dv
    sub = seqs // parts
    rows = n_kv * sub

    copies = {}
    for index, name in enumerate(names):
        copies[name] = pltpu.make_async_copy(hbm[name], vm[name], local_sem.at[index])
    for name in names[:EARLY]:
        copies[name].start()

    barrier = pltpu.get_barrier_semaphore()
    for o in range(1, n_kv):
        pl.semaphore_signal(
            barrier, inc=1, device_id={"kv": lax.rem(kv + o, n_kv)}, device_id_type=MESH
        )
    for o in range(1, n_tp):
        pl.semaphore_signal(
            barrier, inc=1, device_id={"tp": lax.rem(tp + o, n_tp)}, device_id_type=MESH
        )

    def gain(name):
        return vm[name][...].astype(f32).reshape(1, -1)

    sem_next = [0]
    sends = []

    def claim(number):
        first = sem_next[0]
        sem_next[0] += number
        return first

    def described(src, dst, axis, target, sent, received):
        return pltpu.make_async_remote_copy(
            src_ref=src,
            dst_ref=dst,
            send_sem=send_sem.at[sent],
            recv_sem=recv_sem.at[received],
            device_id={axis: target},
            device_id_type=MESH,
        )

    def remote(src, dst, axis, target):
        index = claim(1)
        copy = described(src, dst, axis, target, index, index)
        copy.start()
        sends.append((None, copy))
        return copy

    line = n_kv == 4 and n_tp % 2 == 0
    paired = lax.rem(tp, 2) == 1
    outer = lax.rem(kv, 3) == 0
    inner = lax.rem(kv, 3) != 0
    side = kv // 2
    partner = kv + 1 - 2 * lax.rem(kv, 2)
    far_inner = 2 - side
    far_outer = 3 - 3 * side

    def when(condition, action):
        if condition is None:
            action()
        else:
            pl.when(condition)(action)

    def launch(condition, copy):
        when(condition, copy.start)
        sends.append((condition, copy))

    paired_outer = jnp.logical_and(paired, outer)
    paired_inner = jnp.logical_and(paired, inner)
    single = jnp.logical_not(paired)

    def sum_start(send, recv, merge, merged):
        if not line or not merged:
            return (scatter(send, recv), None)
        base = claim(5)
        launch(
            paired_outer,
            described(send.at[far_outer], merge.at[0], "kv", partner, base + 1, base + 1),
        )
        launch(
            paired_outer,
            described(send.at[far_inner], merge.at[1], "kv", partner, base + 2, base + 2),
        )
        launch(paired, described(send.at[partner], recv.at[0], "kv", partner, base, base))
        for index, o in enumerate(far_first(n_kv)):
            target = lax.rem(kv + o, n_kv)
            launch(
                single,
                described(send.at[target], recv.at[o - 1], "kv", target, base + index, base + o - 1),
            )
        return (base, (send, recv, merge))

    def sum_merge(started):
        base, refs = started
        if refs is None:
            return
        send, recv, merge = refs

        def step(slot, target, sent):
            described(merge.at[slot], merge.at[slot], "kv", partner, 0, base + 1 + slot).wait_recv()
            total = send[target].astype(f32) + merge[slot].astype(f32)
            send[target] = total.astype(bf16)
            described(send.at[target], recv.at[1], "kv", target, sent, base + 3).start()

        def both():
            step(0, far_outer, base + 3)
            step(1, far_inner, base + 4)

        when(paired_inner, both)
        for target, sent in ((far_outer, base + 3), (far_inner, base + 4)):
            copy = described(send.at[target], recv.at[1], "kv", target, sent, base + 3)
            sends.append((paired_inner, copy))

    def sum_wait(started):
        base, refs = started
        if refs is None:
            wait_all(base)
            return
        send, recv, merge = refs

        def pair():
            for slot, received in ((0, base), (1, base + 3)):
                described(recv.at[slot], recv.at[slot], "kv", partner, 0, received).wait_recv()

        def each():
            for slot in range(n_kv - 1):
                described(recv.at[slot], recv.at[slot], "kv", partner, 0, base + slot).wait_recv()

        when(paired, pair)
        when(single, each)

    def spread_start(buffer, relayed):
        if not line or not relayed:
            return (gather(buffer, "kv"), None)
        base = claim(5)

        def sent_to(condition, target, sent, received):
            copy = described(buffer.at[kv], buffer.at[kv], "kv", target, sent, received)
            launch(condition, copy)

        sent_to(paired_outer, far_inner, base + 1, base + 1)
        sent_to(paired_inner, far_inner, base + 1, base + 2)
        sent_to(paired, partner, base, base)
        for index, o in enumerate(far_first(n_kv)):
            sent_to(single, lax.rem(kv + o, n_kv), base + index, base + o - 1)
        return (base, buffer)

    def landed(buffer, owner, received):
        described(buffer.at[owner], buffer.at[owner], "kv", partner, 0, received).wait_recv()

    def spread_pass(started):
        base, buffer = started
        if buffer is None:
            return

        def passed(owner, sent, received):
            return described(buffer.at[owner], buffer.at[owner], "kv", partner, sent, received)

        hops = (passed(far_inner, base + 4, base + 2), passed(far_outer, base + 3, base + 1))

        def both():
            landed(buffer, far_inner, base + 2)
            hops[0].start()
            landed(buffer, far_outer, base + 1)
            hops[1].start()

        when(paired_inner, both)
        sends.extend((paired_inner, copy) for copy in hops)

    def spread_wait(started):
        base, buffer = started
        if buffer is None:
            wait_all(base)
            return

        def far():
            landed(buffer, far_inner, base + 2)
            landed(buffer, far_outer, base + 1)

        def each():
            for o in range(1, n_kv):
                landed(buffer, lax.rem(kv + n_kv - o, n_kv), base + o - 1)

        when(paired, lambda: landed(buffer, partner, base))
        when(paired_outer, far)
        when(single, each)

    def scatter(send, recv):
        result = []
        for o in far_first(n_kv):
            target = lax.rem(kv + o, n_kv)
            result.append(remote(send.at[target], recv.at[o - 1], "kv", target))
        return result

    def gather_tp(buffer):
        if n_tp % 2:
            return gather(buffer, "tp")
        base = claim(n_tp - 1)
        orders = []
        for me in range(2):
            orders.append(sorted(range(1, n_tp), key=lambda o: (me + o in (0, 1, n_tp), (me + o) % 2, o)))
        for even, odd in zip(*orders):
            o = even + (odd - even) * lax.rem(tp, 2)
            target = lax.rem(tp + o, n_tp)
            sem = base + o - 1
            launch(None, described(buffer.at[tp], buffer.at[tp], "tp", target, sem, sem))
        return [
            described(buffer.at[tp], buffer.at[lax.rem(tp + n_tp - o, n_tp)], "tp", tp, 0, base + o - 1)
            for o in range(1, n_tp)
        ]

    def gather(buffer, axis):
        me, n = (kv, n_kv) if axis == "kv" else (tp, n_tp)
        return [
            remote(buffer.at[me], buffer.at[me], axis, lax.rem(me + o, n)) for o in far_first(n)
        ]

    def wait_all(started):
        for copy in started:
            copy.wait_recv()

    def store_all(buffer, lo, value):
        for p in range(parts):
            for d in range(n_kv):
                first = d * seqs + p * sub
                buffer[p, d, :, lo : lo + value.shape[1]] = value[first : first + sub]

    def store_rows(buffer, p, lo, value):
        for d in range(n_kv):
            buffer[p, d, :, lo : lo + value.shape[1]] = value[d * sub : (d + 1) * sub]

    def rows_of(value, p):
        pieces = [value[d * seqs + p * sub : d * seqs + (p + 1) * sub] for d in range(n_kv)]
        return jnp.concatenate(pieces, axis=0)

    def joined(block):
        return block.astype(f32).reshape(rows, block.shape[2]).astype(bf16)

    def reduced(send, recv, p, lo, hi):
        total = send[p, kv, :, lo:hi].astype(f32)
        for o in range(n_kv - 1):
            total = total + recv[p, o, :, lo:hi].astype(f32)
        return total

    if line:

        @pl.when(paired)
        def _():
            for buffer, chosen in ((a_recv, MERGE_A), (b_recv, MERGE_B)):
                for p in chosen:
                    buffer[p, n_kv - 2] = jnp.zeros(buffer.shape[2:], bf16)
            for buffer in gu_recv:
                for p in MERGE_GU:
                    buffer[p, n_kv - 2] = jnp.zeros(buffer.shape[2:], bf16)

    copies["tokens"].wait()
    copies["g_mix"].wait()
    inputs = vm["tokens"][...].astype(f32)
    scaled = (inputs * gain("g_mix")).astype(bf16)
    store_all(a_send, 3 * kw, split_hi_lo(jnp.sum(inputs * inputs, axis=1, keepdims=True)))
    for index, name in enumerate(("w_query", "w_key", "w_decay")):
        copies[name].wait()
        part = jnp.dot(scaled, vm[name][...], preferred_element_type=f32)
        store_all(a_send, index * kw, part.astype(bf16))
    for name in names[EARLY:]:
        copies[name].start()
    pl.semaphore_wait(barrier, n_kv - 1 + n_tp - 1)
    if line and HOLD:

        @pl.when(paired)
        def _():
            pl.delay(HOLD)

    def start_a(p):
        return sum_start(a_send.at[p], a_recv.at[p], a_merge.at[p], p in MERGE_A)

    def start_b(p):
        return sum_start(b_send.at[p], b_recv.at[p], b_merge.at[p], p in MERGE_B)

    sent_a = [start_a(0)]
    for index, name in enumerate(("w_value", "w_outgate")):
        copies[name].wait()
        part = jnp.dot(scaled, vm[name][...], preferred_element_type=f32)
        store_all(b_send, index * vw, part.astype(bf16))
    sent_b = [start_b(0)]
    for p in range(1, parts):
        sent_a.append(start_a(p))
        sent_b.append(start_b(p))

    copies["cum_decay"].wait()
    copies["state"].wait()
    ordinal = lax.broadcasted_iota(jnp.int32, (block_len, dk), 0)

    group = 8 if sub % 8 == 0 else sub

    def prepare(step, carry):
        base = pl.multiple_of(step * group, group)
        for h in range(heads):
            ends = []
            for inner in range(group):
                s = base + inner
                live = lax.rem(lengths[s], block_len)
                picked = jnp.where(ordinal == live - 1, vm["cum_decay"][s, h], 0.0)
                ends.append(jnp.sum(picked, axis=0, keepdims=True))
                state_bf[s, h] = vm["state"][s, h].astype(bf16)
            td_base[pl.ds(base, group), h * dk : (h + 1) * dk] = jnp.concatenate(ends, axis=0)
        return carry

    lax.fori_loop(0, seqs // group, prepare, 0)
    for name in ("step_decay", "key_block", "value_block", "g_heads"):
        copies[name].wait()

    live_ordinal = lax.broadcasted_iota(jnp.int32, (block_len, 1), 0)

    def attend(step, carry):
        base = pl.multiple_of(step * group, group)
        for h in range(heads):
            cols = slice(h * dk, (h + 1) * dk)
            qs = q_ref[pl.ds(base, group), cols]
            tds = td_ref[pl.ds(base, group), cols]
            qes = qe_ref[pl.ds(base, group), cols]
            outs = []
            for inner in range(group):
                s = base + inner
                live = lax.rem(lengths[s], block_len)
                left = jnp.broadcast_to(qes[inner : inner + 1], (16, dk)).astype(bf16)
                carried = jnp.dot(left, state_bf[s, h], preferred_element_type=f32)[:1]
                scores = jnp.sum(
                    qs[inner : inner + 1]
                    * vm["key_block"][s, h].astype(f32)
                    * jnp.exp(tds[inner : inner + 1] - vm["cum_decay"][s, h]),
                    axis=1,
                    keepdims=True,
                )
                scores = jnp.where(live_ordinal < live, scores, 0.0)
                in_block = jnp.sum(
                    scores * vm["value_block"][s, h].astype(f32), axis=0, keepdims=True
                )
                outs.append(carried + in_block)
            head_ref[pl.ds(base, group), h * dv : (h + 1) * dv] = jnp.concatenate(outs, axis=0)
        return carry

    for p in range(parts):
        sum_merge(sent_a[p])
        sum_merge(sent_b[p])
    sent_mixed = []
    for p in range(parts):
        own_rows = slice(p * sub, (p + 1) * sub)
        sum_wait(sent_a[p])
        square = join_hi_lo(reduced(a_send, a_recv, p, 3 * kw, 3 * kw + LANES))
        inverse = lax.rsqrt(square / width + epsilon)
        query = reduced(a_send, a_recv, p, 0, kw) * inverse * dk ** (-0.5)
        keys_new = reduced(a_send, a_recv, p, kw, 2 * kw) * inverse
        decay_pre = reduced(a_send, a_recv, p, 2 * kw, 3 * kw) * inverse
        log_sigmoid = jnp.minimum(decay_pre, 0.0) - jnp.log(1.0 + jnp.exp(-jnp.abs(decay_pre)))
        log_step = log_sigmoid / temper + vm["step_decay"][own_rows]
        token_decay = td_base[own_rows] + log_step
        q_ref[own_rows] = query
        td_ref[own_rows] = token_decay
        qe_ref[own_rows] = query * jnp.exp(token_decay)
        lax.fori_loop(p * sub // group, (p + 1) * sub // group, attend, 0)
        sum_wait(sent_b[p])
        for h in range(heads):
            cols = slice(h * dv, (h + 1) * dv)
            keys = slice(h * dk, (h + 1) * dk)
            values_new = reduced(b_send, b_recv, p, h * dv, (h + 1) * dv) * inverse
            out_gate = reduced(b_send, b_recv, p, vw + h * dv, vw + (h + 1) * dv) * inverse
            own = jnp.sum(query[:, keys] * keys_new[:, keys], axis=1, keepdims=True)
            head_out = head_ref[own_rows, cols] + own * values_new
            scale = lax.rsqrt(jnp.mean(head_out * head_out, axis=1, keepdims=True) + epsilon)
            normed = head_out * scale * gain("g_heads")[:, cols]
            mixed_all[p, kv, :, cols] = (normed * silu(out_gate)).astype(bf16)
        sent_mixed.append(gather(mixed_all.at[p], "kv"))

    copies["w_out"].wait()
    sent_attn = []
    for p in range(parts):
        wait_all(sent_mixed[p])
        part = jnp.dot(joined(mixed_all[p]), vm["w_out"][...], preferred_element_type=f32)
        attn_all[p, tp] = part.astype(bf16)
        sent_attn.append(gather_tp(attn_all.at[p]))

    copies["g_ffn"].wait()
    copies["w_gate"].wait()
    copies["w_up"].wait()
    middles = []
    sent_gu = []
    for p in range(parts):
        wait_all(sent_attn[p])
        attention = attn_all[p, 0].astype(f32)
        for t in range(1, n_tp):
            attention = attention + attn_all[p, t].astype(f32)
        middle = (rows_of(inputs, p) + attention).astype(bf16).astype(f32)
        normed_mid = (middle * gain("g_ffn")).astype(bf16)
        middles.append(middle)
        sent_gu.append([])
        for c, (lo, hi) in enumerate(bounds):
            if c == 0:
                square = jnp.sum(middle * middle, axis=1, keepdims=True)
                store_rows(gu_send[c], p, 2 * (hi - lo), split_hi_lo(square))
            for index, name in enumerate(("w_gate", "w_up")):
                part = jnp.dot(normed_mid, vm[name][:, lo:hi], preferred_element_type=f32)
                store_rows(gu_send[c], p, index * (hi - lo), part.astype(bf16))
            refs = (gu_send[c].at[p], gu_recv[c].at[p], gu_merge[c].at[p])
            sent_gu[p].append(sum_start(*refs, p in MERGE_GU))
    order = [(p, c) for p in range(parts) for c in range(len(bounds))]
    ahead = order[len(bounds) :]
    for c in range(len(bounds)):
        sum_merge(sent_gu[0][c])
    sent_hid = [[] for _ in range(parts)]
    passing = []
    for p, c in order:
        lo, hi = bounds[c]
        w = hi - lo
        sum_wait(sent_gu[p][c])
        if c == 0:
            total = join_hi_lo(reduced(gu_send[c], gu_recv[c], p, 2 * w, 2 * w + LANES))
            mid_inverse = lax.rsqrt(total / width + epsilon)
        gate = reduced(gu_send[c], gu_recv[c], p, 0, w) * mid_inverse
        up = reduced(gu_send[c], gu_recv[c], p, w, 2 * w) * mid_inverse
        hid_all[c][p, kv] = (silu(gate) * up).astype(bf16)
        sent_hid[p].append(spread_start(hid_all[c].at[p], p in RELAY))
        passing.append(sent_hid[p][c])
        if ahead:
            q, e = ahead.pop(0)
            sum_merge(sent_gu[q][e])
        elif len(passing) > 1:
            spread_pass(passing.pop(0))
    copies["w_down"].wait()
    sent_down = []
    for p in range(parts):
        if p == parts - 1:
            for started in passing:
                spread_pass(started)
        down = None
        for c, (lo, hi) in enumerate(bounds):
            spread_wait(sent_hid[p][c])
            part = jnp.dot(joined(hid_all[c][p]), vm["w_down"][lo:hi], preferred_element_type=f32)
            down = part if down is None else down + part
        down_all[p, tp] = down.astype(bf16)
        sent_down.append(gather_tp(down_all.at[p]))
    finals = []
    for p in range(parts):
        wait_all(sent_down[p])
        total = down_all[p, 0].astype(f32)
        for t in range(1, n_tp):
            total = total + down_all[p, t].astype(f32)
        finals.append(middles[p] + total)
    ordered = [finals[p][d * sub : (d + 1) * sub] for d in range(n_kv) for p in range(parts)]
    out_ref[...] = jnp.concatenate(ordered, axis=0).astype(bf16)
    for condition, copy in sends:
        when(condition, copy.wait_send)


ORDER = (
    "tokens",
    "g_mix",
    "w_query",
    "w_key",
    "w_decay",
    "w_value",
    "w_outgate",
    "cum_decay",
    "state",
    "step_decay",
    "key_block",
    "value_block",
    "g_heads",
    "w_out",
    "g_ffn",
    "w_gate",
    "w_up",
    "w_down",
)
CHUNKS = 2
PARTS = 2
HOLD = 0
RELAY = (0,)
MERGE_A = (0, 1)
MERGE_B = (0, 1)
MERGE_GU = (0, 1)
EARLY = 7


def body(n_kv, n_tp, lengths, given):
    rows, columns = given["tokens"].shape
    seqs, heads, dk, dv = given["state"].shape
    kw, vw = heads * dk, heads * dv
    hidden = given["w_gate"].shape[1]
    tiles = -(-hidden // LANES)
    chunks = min(CHUNKS, tiles)
    edges = [min(-(-tiles * c // chunks) * LANES, hidden) for c in range(chunks + 1)]
    bounds = tuple(zip(edges[:-1], edges[1:]))
    widths = [hi - lo for lo, hi in bounds]
    gu_widths = [2 * w + (LANES if c == 0 else 0) for c, w in enumerate(widths)]
    out_cols = given["w_out"].shape[1]
    parts = PARTS if seqs % (8 * PARTS) == 0 else 1
    sub = seqs // parts
    each = max(n_kv - 1, 5)
    remote_count = parts * (each * (3 + 2 * chunks) + 2 * (n_tp - 1))
    scratch = [pltpu.VMEM(given[name].shape, given[name].dtype) for name in ORDER]
    scratch += [
        pltpu.VMEM((seqs, kw), f32),
        pltpu.VMEM((seqs, heads, dk, dv), bf16),
        pltpu.VMEM((seqs, kw), f32),
        pltpu.VMEM((seqs, kw), f32),
        pltpu.VMEM((seqs, kw), f32),
        pltpu.VMEM((seqs, vw), f32),
        pltpu.VMEM((parts, n_kv, sub, 3 * kw + LANES), bf16),
        pltpu.VMEM((parts, n_kv - 1, sub, 3 * kw + LANES), bf16),
        pltpu.VMEM((parts, n_kv, sub, 2 * vw), bf16),
        pltpu.VMEM((parts, n_kv - 1, sub, 2 * vw), bf16),
        pltpu.VMEM((parts, 2, sub, 3 * kw + LANES), bf16),
        pltpu.VMEM((parts, 2, sub, 2 * vw), bf16),
        pltpu.VMEM((parts, n_kv, sub, vw), bf16),
        pltpu.VMEM((parts, n_tp, n_kv * sub, out_cols), bf16),
        [pltpu.VMEM((parts, n_kv, sub, w), bf16) for w in gu_widths],
        [pltpu.VMEM((parts, n_kv - 1, sub, w), bf16) for w in gu_widths],
        [pltpu.VMEM((parts, 2, sub, w), bf16) for w in gu_widths],
        [pltpu.VMEM((parts, n_kv, sub, w), bf16) for w in widths],
        pltpu.VMEM((parts, n_tp, n_kv * sub, out_cols), bf16),
        pltpu.SemaphoreType.DMA((len(ORDER),)),
        pltpu.SemaphoreType.DMA((remote_count,)),
        pltpu.SemaphoreType.DMA((remote_count,)),
    ]
    cfg = (n_kv, n_tp, ORDER, bounds, parts)
    return pl.pallas_call(
        functools.partial(kernel, cfg),
        out_shape=pltpu.VMEM((rows, columns), bf16),
        in_specs=[pl.BlockSpec(memory_space=pltpu.SMEM)]
        + [pl.BlockSpec(memory_space=pltpu.HBM)] * len(ORDER),
        out_specs=pl.BlockSpec(memory_space=pltpu.VMEM),
        scratch_shapes=scratch,
        compiler_params=pltpu.CompilerParams(collective_id=0, has_side_effects=True),
        name="layer",
    )(lengths, *[given[name] for name in ORDER])


NAMES = (
    "tokens",
    "lengths",
    "state",
    "key_block",
    "value_block",
    "cum_decay",
    "step_decay",
    "g_mix",
    "w_query",
    "w_key",
    "w_value",
    "w_outgate",
    "w_decay",
    "g_heads",
    "w_out",
    "g_ffn",
    "w_gate",
    "w_up",
    "w_down",
)


def solution(mesh):
    def call(*arrays):
        given = dict(zip(NAMES, arrays))
        lengths = given.pop("lengths")
        return body(mesh.shape["kv"], mesh.shape["tp"], lengths, given)

    return jax.shard_map(
        call,
        mesh=mesh,
        in_specs=(
            P("grp", "kv"),
            P(("grp", "kv")),
            P(("grp", "kv"), "tp", None, None),
            P(("grp", "kv"), "tp", None, None),
            P(("grp", "kv"), "tp", None, None),
            P(("grp", "kv"), "tp", None, None),
            P(("grp", "kv"), "tp"),
            P("kv"),
            P("kv", "tp"),
            P("kv", "tp"),
            P("kv", "tp"),
            P("kv", "tp"),
            P("kv", "tp"),
            P("tp"),
            P("tp", "kv"),
            P("kv"),
            P("kv", "tp"),
            P("kv", "tp"),
            P("tp", "kv"),
        ),
        out_specs=P("grp", "kv"),
        check_vma=False,
    )
```

```python
import functools

import jax
import jax.numpy as jnp
from jax import lax
from jax.experimental import pallas as pl
from jax.experimental.pallas import tpu as pltpu
from jax.sharding import PartitionSpec as P

f32 = jnp.float32
bf16 = jnp.bfloat16
epsilon = 1e-06
temper = 16.0
LANES = 128
MESH = pl.DeviceIdType.MESH


def silu(v):
    return v / (1.0 + jnp.exp(-v))


def far_first(n):
    return sorted(range(1, n), key=lambda o: (-min(o, n - o), -o))


def split_hi_lo(total):
    lane = lax.broadcasted_iota(jnp.int32, (total.shape[0], LANES), 1)
    wide = jnp.broadcast_to(total, (total.shape[0], LANES))
    high = wide.astype(bf16).astype(f32)
    return jnp.where(lane < LANES // 2, high, wide - high).astype(bf16)


def join_hi_lo(block):
    return block[:, :1] + block[:, LANES // 2 : LANES // 2 + 1]


def kernel(
    cfg,
    *refs,
):
    (n_kv, n_tp, names, bounds, parts) = cfg
    count = len(names)
    hbm = dict(zip(names, refs[:count]))
    (lengths_hbm, out_ref, lengths) = refs[count : count + 3]
    rest = refs[count + 3 :]
    vm = dict(zip(names, rest[:count]))
    (
        td_base,
        state_bf,
        q_ref,
        td_ref,
        qe_ref,
        head_ref,
        a_send,
        a_recv,
        b_send,
        b_recv,
        a_merge,
        b_merge,
        mixed_all,
        attn_all,
        gu_send,
        gu_recv,
        gu_merge,
        hid_all,
        down_all,
        local_sem,
        send_sem,
        recv_sem,
    ) = rest[count:]

    kv = lax.axis_index("kv")
    tp = lax.axis_index("tp")
    seqs, heads, dk, dv = vm["state"].shape
    block_len = vm["key_block"].shape[2]
    width = vm["tokens"].shape[1] * n_kv
    kw = heads * dk
    vw = heads * dv
    sub = seqs // parts
    rows = n_kv * sub

    barrier = pltpu.get_barrier_semaphore()
    for o in range(1, n_kv):
        pl.semaphore_signal(
            barrier, inc=1, device_id={"kv": lax.rem(kv + o, n_kv)}, device_id_type=MESH
        )
    for o in range(1, n_tp):
        pl.semaphore_signal(
            barrier, inc=1, device_id={"tp": lax.rem(tp + o, n_tp)}, device_id_type=MESH
        )

    copies = {}
    for index, name in enumerate(names):
        reused = EARLY <= index < EARLY + FIRST
        sem = index if index < EARLY else index - (EARLY if reused else FIRST)
        copies[name] = pltpu.make_async_copy(hbm[name], vm[name], local_sem.at[sem])
    for name in names[:EARLY]:
        copies[name].start()
    copies["lengths"] = pltpu.make_async_copy(lengths_hbm, lengths, local_sem.at[count - FIRST])

    def gain(name):
        return vm[name][...].astype(f32).reshape(1, -1)

    steps = max(2, len(bounds))
    per_recv = 3 * steps + 2 * len(bounds) + 3
    per_send = steps + len(bounds) + 1

    def sum_sems(p, k):
        return (p * per_send + k, p * per_recv + 3 * k)

    def spread_sems(p, c):
        return (p * per_send + steps + c, p * per_recv + 3 * steps + 2 * c)

    def tp_sems(p):
        return (p * per_send + steps + len(bounds), (p + 1) * per_recv - 3)

    def described(src, dst, axis, target, sent, received):
        return pltpu.make_async_remote_copy(
            src_ref=src,
            dst_ref=dst,
            send_sem=send_sem.at[sent],
            recv_sem=recv_sem.at[received],
            device_id={axis: target},
            device_id_type=MESH,
        )

    line = n_kv == 4 and n_tp % 2 == 0
    paired = lax.rem(tp, 2) == 1
    single = lax.rem(tp, 2) == 0
    outer = lax.rem(kv, 3) == 0
    inner = lax.rem(kv, 3) != 0
    side = kv // 2
    partner = kv + 1 - 2 * lax.rem(kv, 2)
    far_inner = 2 - side
    far_outer = 3 - 3 * side
    paired_outer = jnp.logical_and(paired, outer)
    paired_inner = jnp.logical_and(paired, inner)
    drains = []

    def when(condition, action):
        if condition is None:
            action()
        else:
            pl.when(condition)(action)

    def arrived(ref, received):
        described(ref, ref, "kv", partner if line else kv, 0, received).wait_recv()

    def drain_later(condition, ref, sent):
        drains.append((condition, described(ref, ref, "kv", partner if line else kv, sent, 0)))

    def drain():
        for condition, copy in drains:
            when(condition, copy.wait_send)
        drains.clear()

    def sum_start(send, recv, merge, merged, p, k):
        sent, received = sum_sems(p, k)
        merged = merged and line

        def direct():
            for o in far_first(n_kv):
                target = lax.rem(kv + o, n_kv)
                described(send.at[target], recv.at[o - 1], "kv", target, sent, received).start()

        def to_pair(block, ref, sem):
            described(send.at[block], ref, "kv", partner, sent, sem).start()

        def halves():
            to_pair(far_outer, merge.at[0], received + 1)
            to_pair(far_inner, merge.at[1], received + 2)

        if merged:
            when(paired_outer, halves)
            when(paired, lambda: to_pair(partner, recv.at[0], received))
            when(single, direct)
        else:
            direct()
        drain_later(None, recv, sent)
        return (send, recv, merge, merged, sent, received)

    def sum_merge(started):
        send, recv, merge, merged, sent, received = started

        def both():
            for slot, target in ((0, far_outer), (1, far_inner)):
                arrived(merge.at[slot], received + 1 + slot)
                total = send[target].astype(f32) + merge[slot].astype(f32)
                send[target] = total.astype(bf16)
                described(send.at[target], recv.at[1], "kv", target, sent, received).start()

        if merged:
            when(paired_inner, both)

    def sum_wait(started):
        send, recv, merge, merged, sent, received = started
        if merged:
            when(paired, lambda: arrived(recv.at[0:2], received))
            when(single, lambda: arrived(recv, received))
        else:
            arrived(recv, received)

    def spread_start(buffer, relayed, p, c):
        sent, received = spread_sems(p, c)
        relayed = relayed and line

        def own(target, sem):
            described(buffer.at[kv], buffer.at[kv], "kv", target, sent, sem).start()

        def direct():
            for o in far_first(n_kv):
                own(lax.rem(kv + o, n_kv), received)

        def short():
            own(far_inner, received + 1)
            own(partner, received)

        if relayed:
            when(paired, short)
            when(single, direct)
            drain_later(paired_outer, buffer.at[0:2], sent)
            drain_later(paired_inner, buffer, sent)
            drain_later(single, buffer.at[0 : n_kv - 1], sent)
        else:
            direct()
            drain_later(None, buffer.at[0 : n_kv - 1], sent)
        return (buffer, relayed, sent, received)

    def spread_pass(started):
        buffer, relayed, sent, received = started

        def both():
            arrived(buffer.at[0:2], received + 1)
            for owner in (far_inner, far_outer):
                block = buffer.at[owner]
                described(block, block, "kv", partner, sent, received + 1).start()

        if relayed:
            when(paired_inner, both)

    def spread_wait(started):
        buffer, relayed, sent, received = started
        if relayed:
            when(paired, lambda: arrived(buffer.at[0], received))
            when(paired_outer, lambda: arrived(buffer.at[0:2], received + 1))
            when(single, lambda: arrived(buffer.at[0 : n_kv - 1], received))
        else:
            arrived(buffer.at[0 : n_kv - 1], received)

    def gather_tp(buffer, p):
        sent, received = tp_sems(p)
        orders = []
        for me in range(2):
            keys = {o: (me + o in (1, n_tp), (me + o) % 2, o) for o in range(1, n_tp)}
            orders.append(sorted(keys, key=keys.get))
        for even, odd in zip(*orders):
            o = even + (odd - even) * lax.rem(tp, 2) if n_tp % 2 == 0 else even
            target = lax.rem(tp + o, n_tp)
            block = buffer.at[tp]
            described(block, block, "tp", target, sent, received + 2).start()
        drain_later(None, buffer.at[0 : n_tp - 1], sent)

    def gather_wait(buffer, p):
        arrived(buffer.at[0 : n_tp - 1], tp_sems(p)[1] + 2)

    def store_all(buffer, lo, value):
        for p in range(parts):
            for d in range(n_kv):
                first = d * seqs + p * sub
                buffer[p, d, :, lo : lo + value.shape[1]] = value[first : first + sub]

    def store_rows(buffer, p, lo, value):
        for d in range(n_kv):
            buffer[p, d, :, lo : lo + value.shape[1]] = value[d * sub : (d + 1) * sub]

    def rows_of(value, p):
        pieces = [value[d * seqs + p * sub : d * seqs + (p + 1) * sub] for d in range(n_kv)]
        return jnp.concatenate(pieces, axis=0)

    def joined(block):
        return block.astype(f32).reshape(rows, block.shape[2]).astype(bf16)

    def reduced(send, recv, p, lo, hi):
        total = send[p, kv, :, lo:hi].astype(f32)
        for o in range(n_kv - 1):
            total = total + recv[p, o, :, lo:hi].astype(f32)
        return total

    if line:

        @pl.when(paired)
        def _():
            for buffer, chosen in ((a_recv, MERGE_A), (b_recv, MERGE_B)):
                for p in chosen:
                    buffer[p, n_kv - 2] = jnp.zeros(buffer.shape[2:], bf16)
            for buffer in gu_recv:
                for p in MERGE_GU:
                    buffer[p, n_kv - 2] = jnp.zeros(buffer.shape[2:], bf16)

    copies["tokens"].wait()
    copies["g_mix"].wait()
    inputs = vm["tokens"][...].astype(f32)
    scaled = (inputs * gain("g_mix")).astype(bf16)
    store_all(a_send, 3 * kw, split_hi_lo(jnp.sum(inputs * inputs, axis=1, keepdims=True)))
    for index, name in enumerate(("w_query", "w_key", "w_decay")):
        copies[name].wait()
        part = jnp.dot(scaled, vm[name][...], preferred_element_type=f32)
        store_all(a_send, index * kw, part.astype(bf16))
    for name in names[EARLY:]:
        copies[name].start()
    copies["lengths"].start()
    pl.semaphore_wait(barrier, n_kv - 1 + n_tp - 1)
    if line and HOLD:

        @pl.when(paired)
        def _():
            pl.delay(HOLD)

    def start_a(p):
        return sum_start(a_send.at[p], a_recv.at[p], a_merge.at[p], p in MERGE_A, p, 0)

    def start_b(p):
        return sum_start(b_send.at[p], b_recv.at[p], b_merge.at[p], p in MERGE_B, p, 1)

    sent_a = [start_a(0)]
    for index, name in enumerate(("w_value", "w_outgate")):
        copies[name].wait()
        part = jnp.dot(scaled, vm[name][...], preferred_element_type=f32)
        store_all(b_send, index * vw, part.astype(bf16))
    sent_b = [start_b(0)]
    def start_later():
        for p in range(1, parts):
            sent_a.append(start_a(p))
            sent_b.append(start_b(p))

    if LATER == 0:
        start_later()

    copies["cum_decay"].wait()
    copies["state"].wait()
    copies["lengths"].wait()
    ordinal = lax.broadcasted_iota(jnp.int32, (block_len, dk), 0)

    group = 8 if sub % 8 == 0 else sub

    def prepare(step, carry):
        base = pl.multiple_of(step * group, group)
        for h in range(heads):
            ends = []
            for inner in range(group):
                s = base + inner
                live = lax.rem(lengths[s], block_len)
                picked = jnp.where(ordinal == live - 1, vm["cum_decay"][s, h], 0.0)
                ends.append(jnp.sum(picked, axis=0, keepdims=True))
                state_bf[s, h] = vm["state"][s, h].astype(bf16)
            td_base[pl.ds(base, group), h * dk : (h + 1) * dk] = jnp.concatenate(ends, axis=0)
        return carry

    lax.fori_loop(0, seqs // group, prepare, 0)
    if LATER == 1:
        start_later()
    for name in ("step_decay", "key_block", "value_block", "g_heads"):
        copies[name].wait()

    live_ordinal = lax.broadcasted_iota(jnp.int32, (block_len, 1), 0)

    def attend(step, carry):
        base = pl.multiple_of(step * group, group)
        for h in range(heads):
            cols = slice(h * dk, (h + 1) * dk)
            qs = q_ref[pl.ds(base, group), cols]
            tds = td_ref[pl.ds(base, group), cols]
            qes = qe_ref[pl.ds(base, group), cols]
            outs = []
            for inner in range(group):
                s = base + inner
                live = lax.rem(lengths[s], block_len)
                left = jnp.broadcast_to(qes[inner : inner + 1], (16, dk)).astype(bf16)
                carried = jnp.dot(left, state_bf[s, h], preferred_element_type=f32)[:1]
                scores = jnp.sum(
                    qs[inner : inner + 1]
                    * vm["key_block"][s, h].astype(f32)
                    * jnp.exp(tds[inner : inner + 1] - vm["cum_decay"][s, h]),
                    axis=1,
                    keepdims=True,
                )
                scores = jnp.where(live_ordinal < live, scores, 0.0)
                in_block = jnp.sum(
                    scores * vm["value_block"][s, h].astype(f32), axis=0, keepdims=True
                )
                outs.append(carried + in_block)
            head_ref[pl.ds(base, group), h * dv : (h + 1) * dv] = jnp.concatenate(outs, axis=0)
        return carry

    sum_merge(sent_a[0])
    sum_merge(sent_b[0])
    sent_mixed = []
    for p in range(parts):
        own_rows = slice(p * sub, (p + 1) * sub)
        sum_wait(sent_a[p])
        if p == 0:
            if LATER == 2:
                start_later()
        square = join_hi_lo(reduced(a_send, a_recv, p, 3 * kw, 3 * kw + LANES))
        inverse = lax.rsqrt(square / width + epsilon)
        query = reduced(a_send, a_recv, p, 0, kw) * inverse * dk ** (-0.5)
        keys_new = reduced(a_send, a_recv, p, kw, 2 * kw) * inverse
        decay_pre = reduced(a_send, a_recv, p, 2 * kw, 3 * kw) * inverse
        log_sigmoid = jnp.minimum(decay_pre, 0.0) - jnp.log(1.0 + jnp.exp(-jnp.abs(decay_pre)))
        log_step = log_sigmoid / temper + vm["step_decay"][own_rows]
        token_decay = td_base[own_rows] + log_step
        q_ref[own_rows] = query
        td_ref[own_rows] = token_decay
        qe_ref[own_rows] = query * jnp.exp(token_decay)
        lax.fori_loop(p * sub // group, (p + 1) * sub // group, attend, 0)
        sum_wait(sent_b[p])
        for h in range(heads):
            cols = slice(h * dv, (h + 1) * dv)
            keys = slice(h * dk, (h + 1) * dk)
            values_new = reduced(b_send, b_recv, p, h * dv, (h + 1) * dv) * inverse
            out_gate = reduced(b_send, b_recv, p, vw + h * dv, vw + (h + 1) * dv) * inverse
            own = jnp.sum(query[:, keys] * keys_new[:, keys], axis=1, keepdims=True)
            head_out = head_ref[own_rows, cols] + own * values_new
            scale = lax.rsqrt(jnp.mean(head_out * head_out, axis=1, keepdims=True) + epsilon)
            normed = head_out * scale * gain("g_heads")[:, cols]
            mixed_all[p, kv, :, cols] = (normed * silu(out_gate)).astype(bf16)
        sent_mixed.append(spread_start(mixed_all.at[p], False, p, 0))
        if p + 1 < parts:
            sum_merge(sent_a[p + 1])
            sum_merge(sent_b[p + 1])

    copies["w_out"].wait()
    by_chip = n_tp % 2 == 0
    chip = tp // 2
    chips = n_tp // 2
    mine = chips + lax.rem(tp, 2)
    other = chips + 1 - lax.rem(tp, 2)
    beside = tp + 1 - 2 * lax.rem(tp, 2)

    def chip_sum(p, condition):
        there, here = attn_all.at[p, mine], attn_all.at[p, chip]
        sent, received = tp_sems(p)

        def add():
            arrived(attn_all.at[p, other], received)
            both = attn_all[p, mine].astype(f32) + attn_all[p, other].astype(f32)
            attn_all[p, chip] = both.astype(bf16)
            for o in range(1, chips):
                target = lax.rem(tp + 2 * o, n_tp)
                described(here, here, "tp", target, sent, received + 1).start()

        when(condition, add)

    def chip_wait(p):
        if chips > 1:
            arrived(attn_all.at[p, 0 : chips - 1], tp_sems(p)[1] + 1)

    for p in range(parts):
        spread_wait(sent_mixed[p])
        part = jnp.dot(joined(mixed_all[p]), vm["w_out"][...], preferred_element_type=f32)
        attn_all[p, mine if by_chip else tp] = part.astype(bf16)
        if by_chip:
            there = attn_all.at[p, mine]
            sent, received = tp_sems(p)
            described(there, there, "tp", beside, sent, received).start()
            chip_sum(p, single)
        else:
            gather_tp(attn_all.at[p], p)
    if by_chip:
        for p in range(parts):
            chip_sum(p, paired)
    drain()

    copies["g_ffn"].wait()
    copies["w_gate"].wait()
    copies["w_up"].wait()
    middles = []
    sent_gu = []
    for p in range(parts):
        if by_chip:
            chip_wait(p)
            drain_later(None, attn_all.at[p, 0:chips], tp_sems(p)[0])
        else:
            gather_wait(attn_all.at[p], p)
        attention = attn_all[p, 0].astype(f32)
        for t in range(1, chips if by_chip else n_tp):
            attention = attention + attn_all[p, t].astype(f32)
        middle = (rows_of(inputs, p) + attention).astype(bf16).astype(f32)
        normed_mid = (middle * gain("g_ffn")).astype(bf16)
        middles.append(middle)
        sent_gu.append([])
        for c, (lo, hi) in enumerate(bounds):
            if c == 0:
                square = jnp.sum(middle * middle, axis=1, keepdims=True)
                store_rows(gu_send[c], p, 2 * (hi - lo), split_hi_lo(square))
            for index, name in enumerate(("w_gate", "w_up")):
                part = jnp.dot(normed_mid, vm[name][:, lo:hi], preferred_element_type=f32)
                store_rows(gu_send[c], p, index * (hi - lo), part.astype(bf16))
            refs = (gu_send[c].at[p], gu_recv[c].at[p], gu_merge[c].at[p])
            sent_gu[p].append(sum_start(*refs, p in MERGE_GU, p, c))
    gate_drains = len(drains)
    order = [(p, c) for p in range(parts) for c in range(len(bounds))]
    ahead = order[len(bounds) :]
    for c in range(len(bounds)):
        sum_merge(sent_gu[0][c])
    sent_hid = [[] for _ in range(parts)]
    passing = []
    for p, c in order:
        lo, hi = bounds[c]
        w = hi - lo
        sum_wait(sent_gu[p][c])
        if c == 0:
            total = join_hi_lo(reduced(gu_send[c], gu_recv[c], p, 2 * w, 2 * w + LANES))
            mid_inverse = lax.rsqrt(total / width + epsilon)
        gate = reduced(gu_send[c], gu_recv[c], p, 0, w) * mid_inverse
        up = reduced(gu_send[c], gu_recv[c], p, w, 2 * w) * mid_inverse
        hid_all[c][p, kv] = (silu(gate) * up).astype(bf16)
        sent_hid[p].append(spread_start(hid_all[c].at[p], p in RELAY, p, c))
        passing.append(sent_hid[p][c])
        if ahead:
            q, e = ahead.pop(0)
            sum_merge(sent_gu[q][e])
        elif len(passing) > 1:
            spread_pass(passing.pop(0))
    copies["w_down"].wait()
    held = drains[:]
    drains.clear()
    for condition, copy in held[:gate_drains]:
        when(condition, copy.wait_send)
    for p in range(parts):
        if p == parts - 1:
            for started in passing:
                spread_pass(started)
        down = None
        for c, (lo, hi) in enumerate(bounds):
            spread_wait(sent_hid[p][c])
            part = jnp.dot(joined(hid_all[c][p]), vm["w_down"][lo:hi], preferred_element_type=f32)
            down = part if down is None else down + part
        down_all[p, tp] = down.astype(bf16)
        gather_tp(down_all.at[p], p)
    for condition, copy in held[gate_drains:]:
        when(condition, copy.wait_send)
    finals = []
    for p in range(parts):
        gather_wait(down_all.at[p], p)
        total = down_all[p, 0].astype(f32)
        for t in range(1, n_tp):
            total = total + down_all[p, t].astype(f32)
        finals.append(middles[p] + total)
    ordered = [finals[p][d * sub : (d + 1) * sub] for d in range(n_kv) for p in range(parts)]
    out_ref[...] = jnp.concatenate(ordered, axis=0).astype(bf16)
    drain()


ORDER = (
    "tokens",
    "g_mix",
    "w_query",
    "w_key",
    "w_decay",
    "w_value",
    "w_outgate",
    "cum_decay",
    "state",
    "step_decay",
    "key_block",
    "value_block",
    "g_heads",
    "w_out",
    "g_ffn",
    "w_gate",
    "w_up",
    "w_down",
)
CHUNKS = 2
PARTS = 2
HOLD = 0
LATER = 0
RELAY = (0,)
MERGE_A = (1,)
MERGE_B = (1,)
MERGE_GU = (0, 1)
EARLY = 7
FIRST = 5


def body(n_kv, n_tp, lengths, given):
    rows, columns = given["tokens"].shape
    seqs, heads, dk, dv = given["state"].shape
    kw, vw = heads * dk, heads * dv
    hidden = given["w_gate"].shape[1]
    tiles = -(-hidden // LANES)
    chunks = min(CHUNKS, tiles)
    edges = [min(-(-tiles * c // chunks) * LANES, hidden) for c in range(chunks + 1)]
    bounds = tuple(zip(edges[:-1], edges[1:]))
    widths = [hi - lo for lo, hi in bounds]
    gu_widths = [2 * w + (LANES if c == 0 else 0) for c, w in enumerate(widths)]
    out_cols = given["w_out"].shape[1]
    parts = PARTS if seqs % (8 * PARTS) == 0 else 1
    sub = seqs // parts
    scratch = [pltpu.SMEM(lengths.shape, lengths.dtype)]
    scratch += [pltpu.VMEM(given[name].shape, given[name].dtype) for name in ORDER]
    scratch += [
        pltpu.VMEM((seqs, kw), f32),
        pltpu.VMEM((seqs, heads, dk, dv), bf16),
        pltpu.VMEM((seqs, kw), f32),
        pltpu.VMEM((seqs, kw), f32),
        pltpu.VMEM((seqs, kw), f32),
        pltpu.VMEM((seqs, vw), f32),
        pltpu.VMEM((parts, n_kv, sub, 3 * kw + LANES), bf16),
        pltpu.VMEM((parts, n_kv - 1, sub, 3 * kw + LANES), bf16),
        pltpu.VMEM((parts, n_kv, sub, 2 * vw), bf16),
        pltpu.VMEM((parts, n_kv - 1, sub, 2 * vw), bf16),
        pltpu.VMEM((parts, 2, sub, 3 * kw + LANES), bf16),
        pltpu.VMEM((parts, 2, sub, 2 * vw), bf16),
        pltpu.VMEM((parts, n_kv, sub, vw), bf16),
        pltpu.VMEM((parts, max(n_tp, n_tp // 2 + 2), n_kv * sub, out_cols), bf16),
        [pltpu.VMEM((parts, n_kv, sub, w), bf16) for w in gu_widths],
        [pltpu.VMEM((parts, n_kv - 1, sub, w), bf16) for w in gu_widths],
        [pltpu.VMEM((parts, 2, sub, w), bf16) for w in gu_widths],
        [pltpu.VMEM((parts, n_kv, sub, w), bf16) for w in widths],
        pltpu.VMEM((parts, n_tp, n_kv * sub, out_cols), bf16),
        pltpu.SemaphoreType.DMA((len(ORDER) + 1 - FIRST,)),
        pltpu.SemaphoreType.DMA((parts * (max(2, chunks) + chunks + 1),)),
        pltpu.SemaphoreType.DMA((parts * (3 * max(2, chunks) + 2 * chunks + 3),)),
    ]
    cfg = (n_kv, n_tp, ORDER, bounds, parts)
    return pl.pallas_call(
        functools.partial(kernel, cfg),
        out_shape=pltpu.VMEM((rows, columns), bf16),
        in_specs=[pl.BlockSpec(memory_space=pltpu.HBM)] * (len(ORDER) + 1),
        out_specs=pl.BlockSpec(memory_space=pltpu.VMEM),
        scratch_shapes=scratch,
        compiler_params=pltpu.CompilerParams(collective_id=0, has_side_effects=True),
        name="layer",
    )(*[given[name] for name in ORDER], lengths)


NAMES = (
    "tokens",
    "lengths",
    "state",
    "key_block",
    "value_block",
    "cum_decay",
    "step_decay",
    "g_mix",
    "w_query",
    "w_key",
    "w_value",
    "w_outgate",
    "w_decay",
    "g_heads",
    "w_out",
    "g_ffn",
    "w_gate",
    "w_up",
    "w_down",
)


def solution(mesh):
    def call(*arrays):
        given = dict(zip(NAMES, arrays))
        lengths = given.pop("lengths")
        return body(mesh.shape["kv"], mesh.shape["tp"], lengths, given)

    return jax.shard_map(
        call,
        mesh=mesh,
        in_specs=(
            P("grp", "kv"),
            P(("grp", "kv")),
            P(("grp", "kv"), "tp", None, None),
            P(("grp", "kv"), "tp", None, None),
            P(("grp", "kv"), "tp", None, None),
            P(("grp", "kv"), "tp", None, None),
            P(("grp", "kv"), "tp"),
            P("kv"),
            P("kv", "tp"),
            P("kv", "tp"),
            P("kv", "tp"),
            P("kv", "tp"),
            P("kv", "tp"),
            P("tp"),
            P("tp", "kv"),
            P("kv"),
            P("kv", "tp"),
            P("kv", "tp"),
            P("tp", "kv"),
        ),
        out_specs=P("grp", "kv"),
        check_vma=False,
    )
```

```python
import functools

import jax
import jax.numpy as jnp
from jax import lax
from jax.experimental import pallas as pl
from jax.experimental.pallas import tpu as pltpu
from jax.sharding import PartitionSpec as P

f32 = jnp.float32
bf16 = jnp.bfloat16
epsilon = 1e-06
temper = 16.0
LANES = 128
MESH = pl.DeviceIdType.MESH


def silu(v):
    return v / (1.0 + jnp.exp(-v))


def far_first(n):
    return sorted(range(1, n), key=lambda o: (-min(o, n - o), -o))


def split_hi_lo(total):
    lane = lax.broadcasted_iota(jnp.int32, (total.shape[0], LANES), 1)
    wide = jnp.broadcast_to(total, (total.shape[0], LANES))
    high = wide.astype(bf16).astype(f32)
    return jnp.where(lane < LANES // 2, high, wide - high).astype(bf16)


def join_hi_lo(block):
    return block[:, :1] + block[:, LANES // 2 : LANES // 2 + 1]


def kernel(
    cfg,
    *refs,
):
    (n_kv, n_tp, names, bounds, parts) = cfg
    count = len(names)
    hbm = dict(zip(names, refs[:count]))
    (lengths_hbm, out_ref, lengths) = refs[count : count + 3]
    rest = refs[count + 3 :]
    vm = dict(zip(names, rest[:count]))
    (
        td_base,
        state_bf,
        q_ref,
        td_ref,
        qe_ref,
        head_ref,
        a_send,
        a_recv,
        b_send,
        b_recv,
        a_merge,
        b_merge,
        mixed_all,
        attn_all,
        gu_send,
        gu_recv,
        gu_merge,
        hid_all,
        down_all,
        local_sem,
        send_sem,
        recv_sem,
    ) = rest[count:]

    kv = lax.axis_index("kv")
    tp = lax.axis_index("tp")
    seqs, heads, dk, dv = vm["state"].shape
    block_len = vm["key_block"].shape[2]
    width = vm["tokens"].shape[1] * n_kv
    kw = heads * dk
    vw = heads * dv
    sub = seqs // parts
    rows = n_kv * sub

    barrier = pltpu.get_barrier_semaphore()
    for o in range(1, n_kv):
        pl.semaphore_signal(
            barrier, inc=1, device_id={"kv": lax.rem(kv + o, n_kv)}, device_id_type=MESH
        )
    for o in range(1, n_tp):
        pl.semaphore_signal(
            barrier, inc=1, device_id={"tp": lax.rem(tp + o, n_tp)}, device_id_type=MESH
        )

    copies = {}
    for index, name in enumerate(names):
        reused = EARLY <= index < EARLY + FIRST
        sem = index if index < EARLY else index - (EARLY if reused else FIRST)
        copies[name] = pltpu.make_async_copy(hbm[name], vm[name], local_sem.at[sem])
    for name in names[:EARLY]:
        copies[name].start()
    copies["lengths"] = pltpu.make_async_copy(lengths_hbm, lengths, local_sem.at[count - FIRST])

    def gain(name):
        return vm[name][...].astype(f32).reshape(1, -1)

    steps = max(2, len(bounds))
    per_recv = 3 * steps + 2 * len(bounds) + 3
    per_send = steps + len(bounds) + 1

    def sum_sems(p, k):
        return (p * per_send + k, p * per_recv + 3 * k)

    def spread_sems(p, c):
        return (p * per_send + steps + c, p * per_recv + 3 * steps + 2 * c)

    def tp_sems(p):
        return (p * per_send + steps + len(bounds), (p + 1) * per_recv - 3)

    def described(src, dst, axis, target, sent, received):
        return pltpu.make_async_remote_copy(
            src_ref=src,
            dst_ref=dst,
            send_sem=send_sem.at[sent],
            recv_sem=recv_sem.at[received],
            device_id={axis: target},
            device_id_type=MESH,
        )

    line = n_kv == 4 and n_tp % 2 == 0
    paired = lax.rem(tp, 2) == 1
    single = lax.rem(tp, 2) == 0
    outer = lax.rem(kv, 3) == 0
    inner = lax.rem(kv, 3) != 0
    side = kv // 2
    partner = kv + 1 - 2 * lax.rem(kv, 2)
    far_inner = 2 - side
    far_outer = 3 - 3 * side
    paired_outer = jnp.logical_and(paired, outer)
    paired_inner = jnp.logical_and(paired, inner)
    drains = []

    def when(condition, action):
        if condition is None:
            action()
        else:
            pl.when(condition)(action)

    def arrived(ref, received):
        described(ref, ref, "kv", partner if line else kv, 0, received).wait_recv()

    def drain_later(condition, ref, sent):
        drains.append((condition, described(ref, ref, "kv", partner if line else kv, sent, 0)))

    def drain():
        for condition, copy in drains:
            when(condition, copy.wait_send)
        drains.clear()

    def targets():
        if line and FAR:
            return (far_outer, far_inner, partner)
        return tuple(lax.rem(kv + o, n_kv) for o in far_first(n_kv))

    def sum_start(send, recv, merge, merged, p, k, who=None):
        sent, received = sum_sems(p, k)
        merged = merged and line

        def direct():
            for target in targets():
                slot = lax.rem(target - kv + n_kv, n_kv) - 1
                described(send.at[target], recv.at[slot], "kv", target, sent, received).start()

        def to_pair(block, ref, sem):
            described(send.at[block], ref, "kv", partner, sent, sem).start()

        def halves():
            to_pair(far_outer, merge.at[0], received + 1)
            to_pair(far_inner, merge.at[1], received + 2)

        if merged:
            if who is not single:
                when(paired_outer, halves)
                when(paired, lambda: to_pair(partner, recv.at[0], received))
            if who is not paired:
                when(single, direct)
        else:
            when(who, direct)
        if who is not single:
            drain_later(None, recv, sent)
        return (send, recv, merge, merged, sent, received)

    def sum_merge(started):
        send, recv, merge, merged, sent, received = started

        def both():
            for slot, target in ((0, far_outer), (1, far_inner)):
                arrived(merge.at[slot], received + 1 + slot)
                total = send[target].astype(f32) + merge[slot].astype(f32)
                send[target] = total.astype(bf16)
                described(send.at[target], recv.at[1], "kv", target, sent, received).start()

        if merged:
            when(paired_inner, both)

    def sum_wait(started):
        send, recv, merge, merged, sent, received = started
        if merged:
            when(paired, lambda: arrived(recv.at[0:2], received))
            when(single, lambda: arrived(recv, received))
        else:
            arrived(recv, received)

    def spread_start(buffer, relayed, p, c):
        sent, received = spread_sems(p, c)
        relayed = relayed and line

        def own(target, sem):
            described(buffer.at[kv], buffer.at[kv], "kv", target, sent, sem).start()

        def direct():
            for target in targets():
                own(target, received)

        def short():
            own(far_inner, received + 1)
            own(partner, received)

        if relayed:
            when(paired, short)
            when(single, direct)
            drain_later(paired_outer, buffer.at[0:2], sent)
            drain_later(paired_inner, buffer, sent)
            drain_later(single, buffer.at[0 : n_kv - 1], sent)
        else:
            direct()
            drain_later(None, buffer.at[0 : n_kv - 1], sent)
        return (buffer, relayed, sent, received)

    def spread_pass(started):
        buffer, relayed, sent, received = started

        def both():
            arrived(buffer.at[0:2], received + 1)
            for owner in (far_inner, far_outer):
                block = buffer.at[owner]
                described(block, block, "kv", partner, sent, received + 1).start()

        if relayed:
            when(paired_inner, both)

    def spread_wait(started):
        buffer, relayed, sent, received = started
        if relayed:
            when(paired, lambda: arrived(buffer.at[0], received))
            when(paired_outer, lambda: arrived(buffer.at[0:2], received + 1))
            when(single, lambda: arrived(buffer.at[0 : n_kv - 1], received))
        else:
            arrived(buffer.at[0 : n_kv - 1], received)

    def gather_tp(buffer, p):
        sent, received = tp_sems(p)
        orders = []
        for me in range(2):
            keys = {o: (me + o in (1, n_tp), (me + o) % 2, o) for o in range(1, n_tp)}
            orders.append(sorted(keys, key=keys.get))
        for even, odd in zip(*orders):
            o = even + (odd - even) * lax.rem(tp, 2) if n_tp % 2 == 0 else even
            target = lax.rem(tp + o, n_tp)
            block = buffer.at[tp]
            described(block, block, "tp", target, sent, received + 2).start()
        drain_later(None, buffer.at[0 : n_tp - 1], sent)

    def gather_wait(buffer, p):
        arrived(buffer.at[0 : n_tp - 1], tp_sems(p)[1] + 2)

    def store_all(buffer, lo, value):
        for p in range(parts):
            for d in range(n_kv):
                first = d * seqs + p * sub
                buffer[p, d, :, lo : lo + value.shape[1]] = value[first : first + sub]

    def store_rows(buffer, p, lo, value):
        for d in range(n_kv):
            buffer[p, d, :, lo : lo + value.shape[1]] = value[d * sub : (d + 1) * sub]

    def rows_of(value, p):
        pieces = [value[d * seqs + p * sub : d * seqs + (p + 1) * sub] for d in range(n_kv)]
        return jnp.concatenate(pieces, axis=0)

    def joined(block):
        return block.astype(f32).reshape(rows, block.shape[2]).astype(bf16)

    def reduced(send, recv, p, lo, hi):
        total = send[p, kv, :, lo:hi].astype(f32)
        for o in range(n_kv - 1):
            total = total + recv[p, o, :, lo:hi].astype(f32)
        return total

    if line:

        @pl.when(paired)
        def _():
            for buffer, chosen in ((a_recv, MERGE_A), (b_recv, MERGE_B)):
                for p in chosen:
                    buffer[p, n_kv - 2] = jnp.zeros(buffer.shape[2:], bf16)
            for buffer in gu_recv:
                for p in MERGE_GU:
                    buffer[p, n_kv - 2] = jnp.zeros(buffer.shape[2:], bf16)

    copies["tokens"].wait()
    copies["g_mix"].wait()
    inputs = vm["tokens"][...].astype(f32)
    scaled = (inputs * gain("g_mix")).astype(bf16)
    store_all(a_send, 3 * kw, split_hi_lo(jnp.sum(inputs * inputs, axis=1, keepdims=True)))
    for name in ("w_query", "w_key", "w_decay"):
        copies[name].wait()
    for index, name in enumerate(("w_query", "w_key", "w_decay")):
        part = jnp.dot(scaled, vm[name][...], preferred_element_type=f32)
        store_all(a_send, index * kw, part.astype(bf16))
    for name in names[EARLY:]:
        copies[name].start()
    copies["lengths"].start()
    pl.semaphore_wait(barrier, n_kv - 1 + n_tp - 1)
    def start_a(p, who=None):
        return sum_start(a_send.at[p], a_recv.at[p], a_merge.at[p], p in MERGE_A, p, 0, who)

    def start_b(p, who=None):
        return sum_start(b_send.at[p], b_recv.at[p], b_merge.at[p], p in MERGE_B, p, 1, who)

    sent_a = [start_a(0)]
    for name in ("w_value", "w_outgate"):
        copies[name].wait()
    for index, name in enumerate(("w_value", "w_outgate")):
        part = jnp.dot(scaled, vm[name][...], preferred_element_type=f32)
        store_all(b_send, index * vw, part.astype(bf16))
    first = single if line and YIELD else None
    sent_b = [start_b(0, first if YIELD == 2 else None)]
    for p in range(1, parts):
        sent_a.append(start_a(p, first))
        sent_b.append(start_b(p, first))

    copies["cum_decay"].wait()
    copies["state"].wait()
    copies["lengths"].wait()
    ordinal = lax.broadcasted_iota(jnp.int32, (block_len, dk), 0)

    group = 8 if sub % 8 == 0 else sub

    def prepare(step, carry):
        base = pl.multiple_of(step * group, group)
        for h in range(heads):
            ends = []
            for inner in range(group):
                s = base + inner
                live = lax.rem(lengths[s], block_len)
                picked = jnp.where(ordinal == live - 1, vm["cum_decay"][s, h], 0.0)
                ends.append(jnp.sum(picked, axis=0, keepdims=True))
                state_bf[s, h] = vm["state"][s, h].astype(bf16)
            td_base[pl.ds(base, group), h * dk : (h + 1) * dk] = jnp.concatenate(ends, axis=0)
        return carry

    lax.fori_loop(0, seqs // group, prepare, 0)
    if line and YIELD:
        if YIELD == 2:
            start_b(0, paired)
        for p in range(1, parts):
            start_a(p, paired)
            start_b(p, paired)
    for name in ("step_decay", "key_block", "value_block", "g_heads"):
        copies[name].wait()

    live_ordinal = lax.broadcasted_iota(jnp.int32, (block_len, 1), 0)

    def attend(step, carry):
        base = pl.multiple_of(step * group, group)
        for h in range(heads):
            cols = slice(h * dk, (h + 1) * dk)
            qs = q_ref[pl.ds(base, group), cols]
            tds = td_ref[pl.ds(base, group), cols]
            qes = qe_ref[pl.ds(base, group), cols]
            outs = []
            for inner in range(group):
                s = base + inner
                live = lax.rem(lengths[s], block_len)
                left = jnp.broadcast_to(qes[inner : inner + 1], (16, dk)).astype(bf16)
                carried = jnp.dot(left, state_bf[s, h], preferred_element_type=f32)[:1]
                scores = jnp.sum(
                    qs[inner : inner + 1]
                    * vm["key_block"][s, h].astype(f32)
                    * jnp.exp(tds[inner : inner + 1] - vm["cum_decay"][s, h]),
                    axis=1,
                    keepdims=True,
                )
                scores = jnp.where(live_ordinal < live, scores, 0.0)
                in_block = jnp.sum(
                    scores * vm["value_block"][s, h].astype(f32), axis=0, keepdims=True
                )
                outs.append(carried + in_block)
            head_ref[pl.ds(base, group), h * dv : (h + 1) * dv] = jnp.concatenate(outs, axis=0)
        return carry

    sum_merge(sent_a[0])
    sum_merge(sent_b[0])
    sent_mixed = []
    for p in range(parts):
        own_rows = slice(p * sub, (p + 1) * sub)
        sum_wait(sent_a[p])
        square = join_hi_lo(reduced(a_send, a_recv, p, 3 * kw, 3 * kw + LANES))
        inverse = lax.rsqrt(square / width + epsilon)
        query = reduced(a_send, a_recv, p, 0, kw) * inverse * dk ** (-0.5)
        keys_new = reduced(a_send, a_recv, p, kw, 2 * kw) * inverse
        decay_pre = reduced(a_send, a_recv, p, 2 * kw, 3 * kw) * inverse
        log_sigmoid = jnp.minimum(decay_pre, 0.0) - jnp.log(1.0 + jnp.exp(-jnp.abs(decay_pre)))
        log_step = log_sigmoid / temper + vm["step_decay"][own_rows]
        token_decay = td_base[own_rows] + log_step
        q_ref[own_rows] = query
        td_ref[own_rows] = token_decay
        qe_ref[own_rows] = query * jnp.exp(token_decay)
        lax.fori_loop(p * sub // group, (p + 1) * sub // group, attend, 0)
        sum_wait(sent_b[p])
        for h in range(heads):
            cols = slice(h * dv, (h + 1) * dv)
            keys = slice(h * dk, (h + 1) * dk)
            values_new = reduced(b_send, b_recv, p, h * dv, (h + 1) * dv) * inverse
            out_gate = reduced(b_send, b_recv, p, vw + h * dv, vw + (h + 1) * dv) * inverse
            own = jnp.sum(query[:, keys] * keys_new[:, keys], axis=1, keepdims=True)
            head_out = head_ref[own_rows, cols] + own * values_new
            scale = lax.rsqrt(jnp.mean(head_out * head_out, axis=1, keepdims=True) + epsilon)
            normed = head_out * scale * gain("g_heads")[:, cols]
            mixed_all[p, kv, :, cols] = (normed * silu(out_gate)).astype(bf16)
        sent_mixed.append(spread_start(mixed_all.at[p], False, p, 0))
        if p + 1 < parts:
            sum_merge(sent_a[p + 1])
            sum_merge(sent_b[p + 1])

    copies["w_out"].wait()
    by_chip = n_tp % 2 == 0
    chip = tp // 2
    chips = n_tp // 2
    mine = chips + lax.rem(tp, 2)
    other = chips + 1 - lax.rem(tp, 2)
    beside = tp + 1 - 2 * lax.rem(tp, 2)

    def chip_sum(p, condition):
        there, here = attn_all.at[p, mine], attn_all.at[p, chip]
        sent, received = tp_sems(p)

        def add():
            arrived(attn_all.at[p, other], received)
            both = attn_all[p, mine].astype(f32) + attn_all[p, other].astype(f32)
            attn_all[p, chip] = both.astype(bf16)
            for o in range(1, chips):
                target = lax.rem(tp + 2 * o, n_tp)
                described(here, here, "tp", target, sent, received + 1).start()

        when(condition, add)

    def chip_wait(p):
        if chips > 1:
            arrived(attn_all.at[p, 0 : chips - 1], tp_sems(p)[1] + 1)

    for p in range(parts):
        spread_wait(sent_mixed[p])
        part = jnp.dot(joined(mixed_all[p]), vm["w_out"][...], preferred_element_type=f32)
        attn_all[p, mine if by_chip else tp] = part.astype(bf16)
        if by_chip:
            there = attn_all.at[p, mine]
            sent, received = tp_sems(p)
            described(there, there, "tp", beside, sent, received).start()
            chip_sum(p, single)
        else:
            gather_tp(attn_all.at[p], p)
    if by_chip:
        for p in range(parts):
            chip_sum(p, paired)
    drain()

    copies["g_ffn"].wait()
    copies["w_gate"].wait()
    copies["w_up"].wait()
    middles = []
    sent_gu = []
    for p in range(parts):
        if by_chip:
            chip_wait(p)
            drain_later(None, attn_all.at[p, 0:chips], tp_sems(p)[0])
        else:
            gather_wait(attn_all.at[p], p)
        attention = attn_all[p, 0].astype(f32)
        for t in range(1, chips if by_chip else n_tp):
            attention = attention + attn_all[p, t].astype(f32)
        middle = (rows_of(inputs, p) + attention).astype(bf16).astype(f32)
        normed_mid = (middle * gain("g_ffn")).astype(bf16)
        middles.append(middle)
        sent_gu.append([])
        for c, (lo, hi) in enumerate(bounds):
            if c == 0:
                square = jnp.sum(middle * middle, axis=1, keepdims=True)
                store_rows(gu_send[c], p, 2 * (hi - lo), split_hi_lo(square))
            for index, name in enumerate(("w_gate", "w_up")):
                part = jnp.dot(normed_mid, vm[name][:, lo:hi], preferred_element_type=f32)
                store_rows(gu_send[c], p, index * (hi - lo), part.astype(bf16))
            refs = (gu_send[c].at[p], gu_recv[c].at[p], gu_merge[c].at[p])
            sent_gu[p].append(sum_start(*refs, p in MERGE_GU, p, c))
    gate_drains = len(drains)
    order = [(p, c) for p in range(parts) for c in range(len(bounds))]
    ahead = order[len(bounds) :]
    for c in range(len(bounds)):
        sum_merge(sent_gu[0][c])
    sent_hid = [[] for _ in range(parts)]
    passing = []
    for p, c in order:
        lo, hi = bounds[c]
        w = hi - lo
        sum_wait(sent_gu[p][c])
        if c == 0:
            total = join_hi_lo(reduced(gu_send[c], gu_recv[c], p, 2 * w, 2 * w + LANES))
            mid_inverse = lax.rsqrt(total / width + epsilon)
        gate = reduced(gu_send[c], gu_recv[c], p, 0, w) * mid_inverse
        up = reduced(gu_send[c], gu_recv[c], p, w, 2 * w) * mid_inverse
        hid_all[c][p, kv] = (silu(gate) * up).astype(bf16)
        sent_hid[p].append(spread_start(hid_all[c].at[p], p in RELAY, p, c))
        passing.append(sent_hid[p][c])
        if ahead:
            q, e = ahead.pop(0)
            sum_merge(sent_gu[q][e])
        elif len(passing) > 1:
            spread_pass(passing.pop(0))
    copies["w_down"].wait()
    held = drains[:]
    drains.clear()
    for condition, copy in held[:gate_drains]:
        when(condition, copy.wait_send)
    for p in range(parts):
        if p == parts - 1:
            for started in passing:
                spread_pass(started)
        down = None
        for c, (lo, hi) in enumerate(bounds):
            spread_wait(sent_hid[p][c])
            part = jnp.dot(joined(hid_all[c][p]), vm["w_down"][lo:hi], preferred_element_type=f32)
            down = part if down is None else down + part
        down_all[p, tp] = down.astype(bf16)
        gather_tp(down_all.at[p], p)
    for condition, copy in held[gate_drains:]:
        when(condition, copy.wait_send)
    finals = []
    for p in range(parts):
        gather_wait(down_all.at[p], p)
        total = down_all[p, 0].astype(f32)
        for t in range(1, n_tp):
            total = total + down_all[p, t].astype(f32)
        finals.append(middles[p] + total)
    ordered = [finals[p][d * sub : (d + 1) * sub] for d in range(n_kv) for p in range(parts)]
    out_ref[...] = jnp.concatenate(ordered, axis=0).astype(bf16)
    drain()


ORDER = (
    "tokens",
    "g_mix",
    "w_query",
    "w_key",
    "w_decay",
    "w_value",
    "w_outgate",
    "cum_decay",
    "state",
    "step_decay",
    "key_block",
    "value_block",
    "g_heads",
    "w_out",
    "g_ffn",
    "w_gate",
    "w_up",
    "w_down",
)
CHUNKS = 3
PARTS = 2
YIELD = 0
FAR = True
RELAY = (0,)
MERGE_A = (1,)
MERGE_B = (1,)
MERGE_GU = (0, 1)
EARLY = 7
FIRST = 5


def body(n_kv, n_tp, lengths, given):
    rows, columns = given["tokens"].shape
    seqs, heads, dk, dv = given["state"].shape
    kw, vw = heads * dk, heads * dv
    hidden = given["w_gate"].shape[1]
    tiles = -(-hidden // LANES)
    chunks = min(CHUNKS, tiles)
    edges = [min(-(-tiles * c // chunks) * LANES, hidden) for c in range(chunks + 1)]
    bounds = tuple(zip(edges[:-1], edges[1:]))
    widths = [hi - lo for lo, hi in bounds]
    gu_widths = [2 * w + (LANES if c == 0 else 0) for c, w in enumerate(widths)]
    out_cols = given["w_out"].shape[1]
    parts = PARTS if seqs % (8 * PARTS) == 0 else 1
    sub = seqs // parts
    scratch = [pltpu.SMEM(lengths.shape, lengths.dtype)]
    scratch += [pltpu.VMEM(given[name].shape, given[name].dtype) for name in ORDER]
    scratch += [
        pltpu.VMEM((seqs, kw), f32),
        pltpu.VMEM((seqs, heads, dk, dv), bf16),
        pltpu.VMEM((seqs, kw), f32),
        pltpu.VMEM((seqs, kw), f32),
        pltpu.VMEM((seqs, kw), f32),
        pltpu.VMEM((seqs, vw), f32),
        pltpu.VMEM((parts, n_kv, sub, 3 * kw + LANES), bf16),
        pltpu.VMEM((parts, n_kv - 1, sub, 3 * kw + LANES), bf16),
        pltpu.VMEM((parts, n_kv, sub, 2 * vw), bf16),
        pltpu.VMEM((parts, n_kv - 1, sub, 2 * vw), bf16),
        pltpu.VMEM((parts, 2, sub, 3 * kw + LANES), bf16),
        pltpu.VMEM((parts, 2, sub, 2 * vw), bf16),
        pltpu.VMEM((parts, n_kv, sub, vw), bf16),
        pltpu.VMEM((parts, max(n_tp, n_tp // 2 + 2), n_kv * sub, out_cols), bf16),
        [pltpu.VMEM((parts, n_kv, sub, w), bf16) for w in gu_widths],
        [pltpu.VMEM((parts, n_kv - 1, sub, w), bf16) for w in gu_widths],
        [pltpu.VMEM((parts, 2, sub, w), bf16) for w in gu_widths],
        [pltpu.VMEM((parts, n_kv, sub, w), bf16) for w in widths],
        pltpu.VMEM((parts, n_tp, n_kv * sub, out_cols), bf16),
        pltpu.SemaphoreType.DMA((len(ORDER) + 1 - FIRST,)),
        pltpu.SemaphoreType.DMA((parts * (max(2, chunks) + chunks + 1),)),
        pltpu.SemaphoreType.DMA((parts * (3 * max(2, chunks) + 2 * chunks + 3),)),
    ]
    cfg = (n_kv, n_tp, ORDER, bounds, parts)
    return pl.pallas_call(
        functools.partial(kernel, cfg),
        out_shape=pltpu.VMEM((rows, columns), bf16),
        in_specs=[pl.BlockSpec(memory_space=pltpu.HBM)] * (len(ORDER) + 1),
        out_specs=pl.BlockSpec(memory_space=pltpu.VMEM),
        scratch_shapes=scratch,
        compiler_params=pltpu.CompilerParams(collective_id=0, has_side_effects=True),
        name="layer",
    )(*[given[name] for name in ORDER], lengths)


NAMES = (
    "tokens",
    "lengths",
    "state",
    "key_block",
    "value_block",
    "cum_decay",
    "step_decay",
    "g_mix",
    "w_query",
    "w_key",
    "w_value",
    "w_outgate",
    "w_decay",
    "g_heads",
    "w_out",
    "g_ffn",
    "w_gate",
    "w_up",
    "w_down",
)


def solution(mesh):
    def call(*arrays):
        given = dict(zip(NAMES, arrays))
        lengths = given.pop("lengths")
        return body(mesh.shape["kv"], mesh.shape["tp"], lengths, given)

    return jax.shard_map(
        call,
        mesh=mesh,
        in_specs=(
            P("grp", "kv"),
            P(("grp", "kv")),
            P(("grp", "kv"), "tp", None, None),
            P(("grp", "kv"), "tp", None, None),
            P(("grp", "kv"), "tp", None, None),
            P(("grp", "kv"), "tp", None, None),
            P(("grp", "kv"), "tp"),
            P("kv"),
            P("kv", "tp"),
            P("kv", "tp"),
            P("kv", "tp"),
            P("kv", "tp"),
            P("kv", "tp"),
            P("tp"),
            P("tp", "kv"),
            P("kv"),
            P("kv", "tp"),
            P("kv", "tp"),
            P("tp", "kv"),
        ),
        out_specs=P("grp", "kv"),
        check_vma=False,
    )
```

```python
import functools

import jax
import jax.numpy as jnp
from jax import lax
from jax.experimental import pallas as pl
from jax.experimental.pallas import tpu as pltpu
from jax.sharding import PartitionSpec as P

f32 = jnp.float32
bf16 = jnp.bfloat16
epsilon = 1e-06
temper = 16.0
LANES = 128
MESH = pl.DeviceIdType.MESH


def silu(v):
    return v / (1.0 + jnp.exp(-v))


def far_first(n):
    return sorted(range(1, n), key=lambda o: (-min(o, n - o), -o))


def split_hi_lo(total):
    lane = lax.broadcasted_iota(jnp.int32, (total.shape[0], LANES), 1)
    wide = jnp.broadcast_to(total, (total.shape[0], LANES))
    high = wide.astype(bf16).astype(f32)
    return jnp.where(lane < LANES // 2, high, wide - high).astype(bf16)


def join_hi_lo(block):
    return block[:, :1] + block[:, LANES // 2 : LANES // 2 + 1]


def kernel(
    cfg,
    *refs,
):
    (n_kv, n_tp, names, bounds, parts) = cfg
    count = len(names)
    hbm = dict(zip(names, refs[:count]))
    (lengths_hbm, out_ref, lengths) = refs[count : count + 3]
    rest = refs[count + 3 :]
    vm = dict(zip(names, rest[:count]))
    (
        td_base,
        state_bf,
        q_ref,
        td_ref,
        qe_ref,
        head_ref,
        a_send,
        a_recv,
        b_send,
        b_recv,
        a_merge,
        b_merge,
        mixed_all,
        attn_all,
        gu_send,
        gu_recv,
        gu_merge,
        hid_all,
        down_all,
        local_sem,
        send_sem,
        recv_sem,
    ) = rest[count:]

    kv = lax.axis_index("kv")
    tp = lax.axis_index("tp")
    seqs, heads, dk, dv = vm["state"].shape
    block_len = vm["key_block"].shape[2]
    width = vm["tokens"].shape[1] * n_kv
    kw = heads * dk
    vw = heads * dv
    sub = seqs // parts
    rows = n_kv * sub

    barrier = pltpu.get_barrier_semaphore()
    for o in range(1, n_kv):
        pl.semaphore_signal(
            barrier, inc=1, device_id={"kv": lax.rem(kv + o, n_kv)}, device_id_type=MESH
        )
    for o in range(1, n_tp):
        pl.semaphore_signal(
            barrier, inc=1, device_id={"tp": lax.rem(tp + o, n_tp)}, device_id_type=MESH
        )

    copies = {}
    for index, name in enumerate(names):
        if index >= LAST:
            sem = index - LAST
        elif index >= EARLY + FIRST:
            sem = index - FIRST
        else:
            sem = index % EARLY
        copies[name] = pltpu.make_async_copy(hbm[name], vm[name], local_sem.at[sem])
    for name in names[:EARLY]:
        copies[name].start()
    copies["lengths"] = pltpu.make_async_copy(lengths_hbm, lengths, local_sem.at[LAST - FIRST])

    def gain(name):
        return vm[name][...].astype(f32).reshape(1, -1)

    steps = max(2, len(bounds))
    per_recv = 3 * steps + len(bounds) + 3
    per_send = steps + len(bounds) + 1

    def sum_sems(p, k):
        return (p * per_send + k, p * per_recv + 3 * k)

    def spread_sems(p, c):
        return (p * per_send + steps + c, p * per_recv + 3 * steps + c)

    def tp_sems(p):
        return (p * per_send + steps + len(bounds), (p + 1) * per_recv - 3)

    def described(src, dst, axis, target, sent, received):
        return pltpu.make_async_remote_copy(
            src_ref=src,
            dst_ref=dst,
            send_sem=send_sem.at[sent],
            recv_sem=recv_sem.at[received],
            device_id={axis: target},
            device_id_type=MESH,
        )

    line = n_kv == 4 and n_tp % 2 == 0
    paired = lax.rem(tp, 2) == 1
    single = lax.rem(tp, 2) == 0
    outer = lax.rem(kv, 3) == 0
    inner = lax.rem(kv, 3) != 0
    side = kv // 2
    partner = kv + 1 - 2 * lax.rem(kv, 2)
    far_inner = 2 - side
    far_outer = 3 - 3 * side
    paired_outer = jnp.logical_and(paired, outer)
    paired_inner = jnp.logical_and(paired, inner)
    drains = []

    def when(condition, action):
        if condition is None:
            action()
        else:
            pl.when(condition)(action)

    def arrived(ref, received):
        described(ref, ref, "kv", partner if line else kv, 0, received).wait_recv()

    def drain_later(condition, ref, sent):
        drains.append((condition, described(ref, ref, "kv", partner if line else kv, sent, 0)))

    def drain():
        for condition, copy in drains:
            when(condition, copy.wait_send)
        drains.clear()

    def targets():
        if line and FAR:
            return (far_outer, far_inner, partner)
        return tuple(lax.rem(kv + o, n_kv) for o in far_first(n_kv))

    def sum_start(send, recv, merge, merged, p, k, who=None):
        sent, received = sum_sems(p, k)
        merged = merged and line

        def direct():
            for target in targets():
                slot = lax.rem(target - kv + n_kv, n_kv) - 1
                described(send.at[target], recv.at[slot], "kv", target, sent, received).start()

        def to_pair(block, ref, sem):
            described(send.at[block], ref, "kv", partner, sent, sem).start()

        def halves():
            to_pair(far_outer, merge.at[0], received + 1)
            to_pair(far_inner, merge.at[1], received + 2)

        if merged:
            if who is not single:
                when(paired_outer, halves)
                when(paired, lambda: to_pair(partner, recv.at[0], received))
            if who is not paired:
                when(single, direct)
        else:
            when(who, direct)
        if who is not single:
            drain_later(None, recv, sent)
        return (send, recv, merge, merged, sent, received)

    def sum_merge(started):
        send, recv, merge, merged, sent, received = started

        def both():
            for slot, target in ((0, far_outer), (1, far_inner)):
                arrived(merge.at[slot], received + 1 + slot)
                total = send[target].astype(f32) + merge[slot].astype(f32)
                send[target] = total.astype(bf16)
                described(send.at[target], recv.at[1], "kv", target, sent, received).start()

        if merged:
            when(paired_inner, both)

    def sum_wait(started):
        send, recv, merge, merged, sent, received = started
        if merged:
            when(paired, lambda: arrived(recv.at[0:2], received))
            when(single, lambda: arrived(recv, received))
        else:
            arrived(recv, received)

    def spread_start(buffer, relayed, p, c):
        sent, received = spread_sems(p, c)
        relayed = relayed and line
        passed = parts * per_recv + p * len(bounds) + c

        def own(target, sem):
            described(buffer.at[kv], buffer.at[kv], "kv", target, sent, sem).start()

        def direct():
            for target in targets():
                own(target, received)

        def short():
            own(far_inner, passed)
            own(partner, received)

        if relayed:
            when(paired, short)
            when(single, direct)
            drain_later(paired_outer, buffer.at[0:2], sent)
            drain_later(paired_inner, buffer, sent)
            drain_later(single, buffer.at[0 : n_kv - 1], sent)
        else:
            direct()
            drain_later(None, buffer.at[0 : n_kv - 1], sent)
        return (buffer, relayed, sent, received, passed)

    def spread_pass(started):
        buffer, relayed, sent, received, passed = started

        def both():
            arrived(buffer.at[0:2], passed)
            for owner in (far_inner, far_outer):
                block = buffer.at[owner]
                described(block, block, "kv", partner, sent, passed).start()

        if relayed:
            when(paired_inner, both)

    def spread_wait(started):
        buffer, relayed, sent, received, passed = started
        if relayed:
            when(paired, lambda: arrived(buffer.at[0], received))
            when(paired_outer, lambda: arrived(buffer.at[0:2], passed))
            when(single, lambda: arrived(buffer.at[0 : n_kv - 1], received))
        else:
            arrived(buffer.at[0 : n_kv - 1], received)

    def gather_tp(buffer, p):
        sent, received = tp_sems(p)
        orders = []
        for me in range(2):
            keys = {o: (me + o in (1, n_tp), (me + o) % 2, o) for o in range(1, n_tp)}
            orders.append(sorted(keys, key=keys.get))
        for even, odd in zip(*orders):
            o = even + (odd - even) * lax.rem(tp, 2) if n_tp % 2 == 0 else even
            target = lax.rem(tp + o, n_tp)
            block = buffer.at[tp]
            described(block, block, "tp", target, sent, received + 2).start()
        drain_later(None, buffer.at[0 : n_tp - 1], sent)

    def gather_wait(buffer, p):
        arrived(buffer.at[0 : n_tp - 1], tp_sems(p)[1] + 2)

    def store_all(buffer, lo, value):
        for p in range(parts):
            for d in range(n_kv):
                first = d * seqs + p * sub
                buffer[p, d, :, lo : lo + value.shape[1]] = value[first : first + sub]

    def store_rows(buffer, p, lo, value):
        for d in range(n_kv):
            buffer[p, d, :, lo : lo + value.shape[1]] = value[d * sub : (d + 1) * sub]

    def rows_of(value, p):
        pieces = [value[d * seqs + p * sub : d * seqs + (p + 1) * sub] for d in range(n_kv)]
        return jnp.concatenate(pieces, axis=0)

    def joined(block):
        return block.astype(f32).reshape(rows, block.shape[2]).astype(bf16)

    def reduced(send, recv, p, lo, hi):
        total = send[p, kv, :, lo:hi].astype(f32)
        for o in range(n_kv - 1):
            total = total + recv[p, o, :, lo:hi].astype(f32)
        return total

    if line:

        @pl.when(paired)
        def _():
            for buffer, chosen in ((a_recv, MERGE_A), (b_recv, MERGE_B)):
                for p in chosen:
                    buffer[p, n_kv - 2] = jnp.zeros(buffer.shape[2:], bf16)
            for buffer in gu_recv:
                for p in MERGE_GU:
                    buffer[p, n_kv - 2] = jnp.zeros(buffer.shape[2:], bf16)

    copies["tokens"].wait()
    copies["g_mix"].wait()
    inputs = vm["tokens"][...].astype(f32)
    scaled = (inputs * gain("g_mix")).astype(bf16)
    store_all(a_send, 3 * kw, split_hi_lo(jnp.sum(inputs * inputs, axis=1, keepdims=True)))
    for name in ("w_query", "w_key", "w_decay"):
        copies[name].wait()
    for index, name in enumerate(("w_query", "w_key", "w_decay")):
        part = jnp.dot(scaled, vm[name][...], preferred_element_type=f32)
        store_all(a_send, index * kw, part.astype(bf16))
    for name in names[EARLY:LAST]:
        copies[name].start()
    copies["lengths"].start()
    pl.semaphore_wait(barrier, n_kv - 1 + n_tp - 1)
    def start_a(p, who=None):
        return sum_start(a_send.at[p], a_recv.at[p], a_merge.at[p], p in MERGE_A, p, 0, who)

    def start_b(p, who=None):
        return sum_start(b_send.at[p], b_recv.at[p], b_merge.at[p], p in MERGE_B, p, 1, who)

    sent_a = [start_a(0)]
    for name in ("w_value", "w_outgate"):
        copies[name].wait()
    for index, name in enumerate(("w_value", "w_outgate")):
        part = jnp.dot(scaled, vm[name][...], preferred_element_type=f32)
        store_all(b_send, index * vw, part.astype(bf16))
    first = single if line and YIELD else None
    sent_b = [start_b(0, first if YIELD == 2 else None)]
    for p in range(1, parts):
        sent_a.append(start_a(p, first))
        sent_b.append(start_b(p, first))

    copies["cum_decay"].wait()
    copies["state"].wait()
    copies["lengths"].wait()
    ordinal = lax.broadcasted_iota(jnp.int32, (block_len, dk), 0)

    group = 8 if sub % 8 == 0 else sub

    def prepare(step, carry):
        base = pl.multiple_of(step * group, group)
        for h in range(heads):
            ends = []
            for inner in range(group):
                s = base + inner
                live = lax.rem(lengths[s], block_len)
                picked = jnp.where(ordinal == live - 1, vm["cum_decay"][s, h], 0.0)
                ends.append(jnp.sum(picked, axis=0, keepdims=True))
                state_bf[s, h] = vm["state"][s, h].astype(bf16)
            td_base[pl.ds(base, group), h * dk : (h + 1) * dk] = jnp.concatenate(ends, axis=0)
        return carry

    lax.fori_loop(0, seqs // group, prepare, 0)
    if line and YIELD:
        if YIELD == 2:
            start_b(0, paired)
        for p in range(1, parts):
            start_a(p, paired)
            start_b(p, paired)
    for name in ("step_decay", "key_block", "value_block", "g_heads"):
        copies[name].wait()
    for name in names[LAST:]:
        copies[name].start()

    live_ordinal = lax.broadcasted_iota(jnp.int32, (block_len, 1), 0)

    def attend(step, carry):
        base = pl.multiple_of(step * group, group)
        for h in range(heads):
            cols = slice(h * dk, (h + 1) * dk)
            qs = q_ref[pl.ds(base, group), cols]
            tds = td_ref[pl.ds(base, group), cols]
            qes = qe_ref[pl.ds(base, group), cols]
            outs = []
            for inner in range(group):
                s = base + inner
                live = lax.rem(lengths[s], block_len)
                left = jnp.broadcast_to(qes[inner : inner + 1], (16, dk)).astype(bf16)
                carried = jnp.dot(left, state_bf[s, h], preferred_element_type=f32)[:1]
                scores = jnp.sum(
                    qs[inner : inner + 1]
                    * vm["key_block"][s, h].astype(f32)
                    * jnp.exp(tds[inner : inner + 1] - vm["cum_decay"][s, h]),
                    axis=1,
                    keepdims=True,
                )
                scores = jnp.where(live_ordinal < live, scores, 0.0)
                in_block = jnp.sum(
                    scores * vm["value_block"][s, h].astype(f32), axis=0, keepdims=True
                )
                outs.append(carried + in_block)
            head_ref[pl.ds(base, group), h * dv : (h + 1) * dv] = jnp.concatenate(outs, axis=0)
        return carry

    sum_merge(sent_a[0])
    sum_merge(sent_b[0])
    sent_mixed = []
    for p in range(parts):
        own_rows = slice(p * sub, (p + 1) * sub)
        sum_wait(sent_a[p])
        square = join_hi_lo(reduced(a_send, a_recv, p, 3 * kw, 3 * kw + LANES))
        inverse = lax.rsqrt(square / width + epsilon)
        query = reduced(a_send, a_recv, p, 0, kw) * inverse * dk ** (-0.5)
        keys_new = reduced(a_send, a_recv, p, kw, 2 * kw) * inverse
        decay_pre = reduced(a_send, a_recv, p, 2 * kw, 3 * kw) * inverse
        log_sigmoid = jnp.minimum(decay_pre, 0.0) - jnp.log(1.0 + jnp.exp(-jnp.abs(decay_pre)))
        log_step = log_sigmoid / temper + vm["step_decay"][own_rows]
        token_decay = td_base[own_rows] + log_step
        q_ref[own_rows] = query
        td_ref[own_rows] = token_decay
        qe_ref[own_rows] = query * jnp.exp(token_decay)
        lax.fori_loop(p * sub // group, (p + 1) * sub // group, attend, 0)
        sum_wait(sent_b[p])
        for h in range(heads):
            cols = slice(h * dv, (h + 1) * dv)
            keys = slice(h * dk, (h + 1) * dk)
            values_new = reduced(b_send, b_recv, p, h * dv, (h + 1) * dv) * inverse
            out_gate = reduced(b_send, b_recv, p, vw + h * dv, vw + (h + 1) * dv) * inverse
            own = jnp.sum(query[:, keys] * keys_new[:, keys], axis=1, keepdims=True)
            head_out = head_ref[own_rows, cols] + own * values_new
            scale = lax.rsqrt(jnp.mean(head_out * head_out, axis=1, keepdims=True) + epsilon)
            normed = head_out * scale * gain("g_heads")[:, cols]
            mixed_all[p, kv, :, cols] = (normed * silu(out_gate)).astype(bf16)
        sent_mixed.append(spread_start(mixed_all.at[p], False, p, 0))
        if p + 1 < parts:
            sum_merge(sent_a[p + 1])
            sum_merge(sent_b[p + 1])

    copies["w_out"].wait()
    by_chip = n_tp % 2 == 0
    chip = tp // 2
    chips = n_tp // 2
    mine = chips + lax.rem(tp, 2)
    other = chips + 1 - lax.rem(tp, 2)
    beside = tp + 1 - 2 * lax.rem(tp, 2)

    def chip_sum(p, condition):
        there, here = attn_all.at[p, mine], attn_all.at[p, chip]
        sent, received = tp_sems(p)

        def add():
            arrived(attn_all.at[p, other], received)
            both = attn_all[p, mine].astype(f32) + attn_all[p, other].astype(f32)
            attn_all[p, chip] = both.astype(bf16)
            for o in range(1, chips):
                target = lax.rem(tp + 2 * o, n_tp)
                described(here, here, "tp", target, sent, received + 1).start()

        when(condition, add)

    def chip_wait(p):
        if chips > 1:
            arrived(attn_all.at[p, 0 : chips - 1], tp_sems(p)[1] + 1)

    for p in range(parts):
        spread_wait(sent_mixed[p])
        part = jnp.dot(joined(mixed_all[p]), vm["w_out"][...], preferred_element_type=f32)
        attn_all[p, mine if by_chip else tp] = part.astype(bf16)
        if by_chip:
            there = attn_all.at[p, mine]
            sent, received = tp_sems(p)
            described(there, there, "tp", beside, sent, received).start()
            chip_sum(p, single)
        else:
            gather_tp(attn_all.at[p], p)
    if by_chip:
        for p in range(parts):
            chip_sum(p, paired)
    drain()

    copies["g_ffn"].wait()
    copies["w_gate"].wait()
    copies["w_up"].wait()
    middles = []
    sent_gu = []
    for p in range(parts):
        if by_chip:
            chip_wait(p)
            drain_later(None, attn_all.at[p, 0:chips], tp_sems(p)[0])
        else:
            gather_wait(attn_all.at[p], p)
        attention = attn_all[p, 0].astype(f32)
        for t in range(1, chips if by_chip else n_tp):
            attention = attention + attn_all[p, t].astype(f32)
        middle = (rows_of(inputs, p) + attention).astype(bf16).astype(f32)
        normed_mid = (middle * gain("g_ffn")).astype(bf16)
        middles.append(middle)
        sent_gu.append([])
        for c, (lo, hi) in enumerate(bounds):
            if c == 0:
                square = jnp.sum(middle * middle, axis=1, keepdims=True)
                store_rows(gu_send[c], p, 2 * (hi - lo), split_hi_lo(square))
            for index, name in enumerate(("w_gate", "w_up")):
                part = jnp.dot(normed_mid, vm[name][:, lo:hi], preferred_element_type=f32)
                store_rows(gu_send[c], p, index * (hi - lo), part.astype(bf16))
            refs = (gu_send[c].at[p], gu_recv[c].at[p], gu_merge[c].at[p])
            sent_gu[p].append(sum_start(*refs, p in MERGE_GU, p, c))
    gate_drains = len(drains)
    order = [(p, c) for p in range(parts) for c in range(len(bounds))]
    start = min(len(order), len(bounds) + AHEAD)
    ahead = order[start:]
    for p, c in order[:start]:
        sum_merge(sent_gu[p][c])
    sent_hid = [[] for _ in range(parts)]
    passing = []
    for p, c in order:
        lo, hi = bounds[c]
        w = hi - lo
        sum_wait(sent_gu[p][c])
        if c == 0:
            total = join_hi_lo(reduced(gu_send[c], gu_recv[c], p, 2 * w, 2 * w + LANES))
            mid_inverse = lax.rsqrt(total / width + epsilon)
        gate = reduced(gu_send[c], gu_recv[c], p, 0, w) * mid_inverse
        up = reduced(gu_send[c], gu_recv[c], p, w, 2 * w) * mid_inverse
        hid_all[c][p, kv] = (silu(gate) * up).astype(bf16)
        sent_hid[p].append(spread_start(hid_all[c].at[p], p in RELAY, p, c))
        passing.append(sent_hid[p][c])
        if ahead:
            q, e = ahead.pop(0)
            sum_merge(sent_gu[q][e])
        elif len(passing) > 1:
            spread_pass(passing.pop(0))
    copies["w_down"].wait()
    held = drains[:]
    drains.clear()
    for condition, copy in held[:gate_drains]:
        when(condition, copy.wait_send)
    for p in range(parts):
        if p == parts - 1:
            for started in passing:
                spread_pass(started)
        down = None
        for c, (lo, hi) in enumerate(bounds):
            spread_wait(sent_hid[p][c])
            part = jnp.dot(joined(hid_all[c][p]), vm["w_down"][lo:hi], preferred_element_type=f32)
            down = part if down is None else down + part
        down_all[p, tp] = down.astype(bf16)
        gather_tp(down_all.at[p], p)
    for condition, copy in held[gate_drains:]:
        when(condition, copy.wait_send)
    finals = []
    for p in range(parts):
        gather_wait(down_all.at[p], p)
        total = down_all[p, 0].astype(f32)
        for t in range(1, n_tp):
            total = total + down_all[p, t].astype(f32)
        finals.append(middles[p] + total)
    ordered = [finals[p][d * sub : (d + 1) * sub] for d in range(n_kv) for p in range(parts)]
    out_ref[...] = jnp.concatenate(ordered, axis=0).astype(bf16)
    drain()


ORDER = (
    "tokens",
    "g_mix",
    "w_query",
    "w_key",
    "w_decay",
    "w_value",
    "w_outgate",
    "cum_decay",
    "state",
    "step_decay",
    "key_block",
    "value_block",
    "g_heads",
    "w_out",
    "g_ffn",
    "w_gate",
    "w_up",
    "w_down",
)
SHARES = (3, 5, 3)
AHEAD = 1
PARTS = 2
YIELD = 0
FAR = True
RELAY = (0,)
MERGE_A = (1,)
MERGE_B = (1,)
MERGE_GU = (0, 1)
EARLY = 7
FIRST = 5
LAST = 13


def body(n_kv, n_tp, lengths, given):
    rows, columns = given["tokens"].shape
    seqs, heads, dk, dv = given["state"].shape
    kw, vw = heads * dk, heads * dv
    hidden = given["w_gate"].shape[1]
    tiles = -(-hidden // LANES)
    ends = [sum(SHARES[:c]) for c in range(len(SHARES) + 1)]
    edges = sorted({min(-(-tiles * end // ends[-1]) * LANES, hidden) for end in ends})
    chunks = len(edges) - 1
    bounds = tuple(zip(edges[:-1], edges[1:]))
    widths = [hi - lo for lo, hi in bounds]
    gu_widths = [2 * w + (LANES if c == 0 else 0) for c, w in enumerate(widths)]
    out_cols = given["w_out"].shape[1]
    parts = PARTS if seqs % (8 * PARTS) == 0 else 1
    sub = seqs // parts
    scratch = [pltpu.SMEM(lengths.shape, lengths.dtype)]
    scratch += [pltpu.VMEM(given[name].shape, given[name].dtype) for name in ORDER]
    scratch += [
        pltpu.VMEM((seqs, kw), f32),
        pltpu.VMEM((seqs, heads, dk, dv), bf16),
        pltpu.VMEM((seqs, kw), f32),
        pltpu.VMEM((seqs, kw), f32),
        pltpu.VMEM((seqs, kw), f32),
        pltpu.VMEM((seqs, vw), f32),
        pltpu.VMEM((parts, n_kv, sub, 3 * kw + LANES), bf16),
        pltpu.VMEM((parts, n_kv - 1, sub, 3 * kw + LANES), bf16),
        pltpu.VMEM((parts, n_kv, sub, 2 * vw), bf16),
        pltpu.VMEM((parts, n_kv - 1, sub, 2 * vw), bf16),
        pltpu.VMEM((parts, 2, sub, 3 * kw + LANES), bf16),
        pltpu.VMEM((parts, 2, sub, 2 * vw), bf16),
        pltpu.VMEM((parts, n_kv, sub, vw), bf16),
        pltpu.VMEM((parts, max(n_tp, n_tp // 2 + 2), n_kv * sub, out_cols), bf16),
        [pltpu.VMEM((parts, n_kv, sub, w), bf16) for w in gu_widths],
        [pltpu.VMEM((parts, n_kv - 1, sub, w), bf16) for w in gu_widths],
        [pltpu.VMEM((parts, 2, sub, w), bf16) for w in gu_widths],
        [pltpu.VMEM((parts, n_kv, sub, w), bf16) for w in widths],
        pltpu.VMEM((parts, n_tp, n_kv * sub, out_cols), bf16),
        pltpu.SemaphoreType.DMA((LAST + 1 - FIRST,)),
        pltpu.SemaphoreType.DMA((parts * (max(2, chunks) + chunks + 1),)),
        pltpu.SemaphoreType.DMA((parts * (3 * max(2, chunks) + chunks + 3) + len(RELAY) * chunks,)),
    ]
    cfg = (n_kv, n_tp, ORDER, bounds, parts)
    return pl.pallas_call(
        functools.partial(kernel, cfg),
        out_shape=pltpu.VMEM((rows, columns), bf16),
        in_specs=[pl.BlockSpec(memory_space=pltpu.HBM)] * (len(ORDER) + 1),
        out_specs=pl.BlockSpec(memory_space=pltpu.VMEM),
        scratch_shapes=scratch,
        compiler_params=pltpu.CompilerParams(collective_id=0, has_side_effects=True),
        name="layer",
    )(*[given[name] for name in ORDER], lengths)


NAMES = (
    "tokens",
    "lengths",
    "state",
    "key_block",
    "value_block",
    "cum_decay",
    "step_decay",
    "g_mix",
    "w_query",
    "w_key",
    "w_value",
    "w_outgate",
    "w_decay",
    "g_heads",
    "w_out",
    "g_ffn",
    "w_gate",
    "w_up",
    "w_down",
)


def solution(mesh):
    def call(*arrays):
        given = dict(zip(NAMES, arrays))
        lengths = given.pop("lengths")
        return body(mesh.shape["kv"], mesh.shape["tp"], lengths, given)

    return jax.shard_map(
        call,
        mesh=mesh,
        in_specs=(
            P("grp", "kv"),
            P(("grp", "kv")),
            P(("grp", "kv"), "tp", None, None),
            P(("grp", "kv"), "tp", None, None),
            P(("grp", "kv"), "tp", None, None),
            P(("grp", "kv"), "tp", None, None),
            P(("grp", "kv"), "tp"),
            P("kv"),
            P("kv", "tp"),
            P("kv", "tp"),
            P("kv", "tp"),
            P("kv", "tp"),
            P("kv", "tp"),
            P("tp"),
            P("tp", "kv"),
            P("kv"),
            P("kv", "tp"),
            P("kv", "tp"),
            P("tp", "kv"),
        ),
        out_specs=P("grp", "kv"),
        check_vma=False,
    )
```

```python
import functools

import jax
import jax.numpy as jnp
from jax import lax
from jax.experimental import pallas as pl
from jax.experimental.pallas import tpu as pltpu
from jax.sharding import PartitionSpec as P

f32 = jnp.float32
bf16 = jnp.bfloat16
epsilon = 1e-06
temper = 16.0
LANES = 128
MESH = pl.DeviceIdType.MESH


def silu(v):
    return v / (1.0 + jnp.exp(-v))


def far_first(n):
    return sorted(range(1, n), key=lambda o: (-min(o, n - o), -o))


def split_hi_lo(total):
    lane = lax.broadcasted_iota(jnp.int32, (total.shape[0], LANES), 1)
    wide = jnp.broadcast_to(total, (total.shape[0], LANES))
    high = wide.astype(bf16).astype(f32)
    return jnp.where(lane < LANES // 2, high, wide - high).astype(bf16)


def join_hi_lo(block):
    return block[:, :1] + block[:, LANES // 2 : LANES // 2 + 1]


def kernel(
    cfg,
    *refs,
):
    (n_kv, n_tp, names, bounds, parts) = cfg
    count = len(names)
    hbm = dict(zip(names, refs[:count]))
    (lengths_hbm, out_ref, lengths) = refs[count : count + 3]
    rest = refs[count + 3 :]
    vm = dict(zip(names, rest[:count]))
    (
        td_base,
        state_bf,
        q_ref,
        td_ref,
        qe_ref,
        head_ref,
        a_send,
        a_recv,
        b_send,
        b_recv,
        a_merge,
        b_merge,
        mixed_all,
        attn_all,
        gu_send,
        gu_recv,
        gu_merge,
        hid_all,
        down_all,
        local_sem,
        send_sem,
        recv_sem,
    ) = rest[count:]

    kv = lax.axis_index("kv")
    tp = lax.axis_index("tp")
    seqs, heads, dk, dv = vm["state"].shape
    block_len = vm["key_block"].shape[2]
    width = vm["tokens"].shape[1] * n_kv
    kw = heads * dk
    vw = heads * dv
    sub = seqs // parts
    rows = n_kv * sub

    barrier = pltpu.get_barrier_semaphore()
    for o in range(1, n_kv):
        pl.semaphore_signal(
            barrier, inc=1, device_id={"kv": lax.rem(kv + o, n_kv)}, device_id_type=MESH
        )
    for o in range(1, n_tp):
        pl.semaphore_signal(
            barrier, inc=1, device_id={"tp": lax.rem(tp + o, n_tp)}, device_id_type=MESH
        )

    copies = {}
    for index, name in enumerate(names):
        if index >= LAST:
            sem = index - LAST
        elif index >= EARLY + FIRST:
            sem = index - FIRST
        else:
            sem = index % EARLY
        copies[name] = pltpu.make_async_copy(hbm[name], vm[name], local_sem.at[sem])
    for name in names[:EARLY]:
        copies[name].start()
    copies["lengths"] = pltpu.make_async_copy(lengths_hbm, lengths, local_sem.at[LAST - FIRST])

    def gain(name):
        return vm[name][...].astype(f32).reshape(1, -1)

    steps = max(2, len(bounds))
    per_recv = 3 * steps + len(bounds) + 3
    per_send = steps + len(bounds) + 1

    def sum_sems(p, k):
        return (p * per_send + k, p * per_recv + 3 * k)

    def spread_sems(p, c):
        return (p * per_send + steps + c, p * per_recv + 3 * steps + c)

    def tp_sems(p):
        return (p * per_send + steps + len(bounds), (p + 1) * per_recv - 3)

    def described(src, dst, axis, target, sent, received):
        return pltpu.make_async_remote_copy(
            src_ref=src,
            dst_ref=dst,
            send_sem=send_sem.at[sent],
            recv_sem=recv_sem.at[received],
            device_id={axis: target},
            device_id_type=MESH,
        )

    line = n_kv == 4 and n_tp % 2 == 0
    paired = lax.rem(tp, 2) == 1
    single = lax.rem(tp, 2) == 0
    outer = lax.rem(kv, 3) == 0
    inner = lax.rem(kv, 3) != 0
    side = kv // 2
    partner = kv + 1 - 2 * lax.rem(kv, 2)
    far_inner = 2 - side
    far_outer = 3 - 3 * side
    paired_outer = jnp.logical_and(paired, outer)
    paired_inner = jnp.logical_and(paired, inner)
    drains = []

    def when(condition, action):
        if condition is None:
            action()
        else:
            pl.when(condition)(action)

    def arrived(ref, received):
        described(ref, ref, "kv", partner if line else kv, 0, received).wait_recv()

    def drain_later(condition, ref, sent):
        drains.append((condition, described(ref, ref, "kv", partner if line else kv, sent, 0)))

    def drain():
        for condition, copy in drains:
            when(condition, copy.wait_send)
        drains.clear()

    def targets():
        if line and FAR:
            return (far_outer, far_inner, partner)
        return tuple(lax.rem(kv + o, n_kv) for o in far_first(n_kv))

    def sum_start(send, recv, merge, merged, p, k, who=None):
        sent, received = sum_sems(p, k)
        merged = merged and line

        def direct():
            for target in targets():
                slot = lax.rem(target - kv + n_kv, n_kv) - 1
                described(send.at[target], recv.at[slot], "kv", target, sent, received).start()

        def to_pair(block, ref, sem):
            described(send.at[block], ref, "kv", partner, sent, sem).start()

        def halves():
            to_pair(far_outer, merge.at[0], received + 1)
            to_pair(far_inner, merge.at[1], received + 2)

        if merged:
            if who is not single:
                when(paired_outer, halves)
                when(paired, lambda: to_pair(partner, recv.at[0], received))
            if who is not paired:
                when(single, direct)
        else:
            when(who, direct)
        if who is not single:
            drain_later(None, recv, sent)
        return (send, recv, merge, merged, sent, received)

    def sum_merge(started):
        send, recv, merge, merged, sent, received = started

        def both():
            for slot, target in ((0, far_outer), (1, far_inner)):
                arrived(merge.at[slot], received + 1 + slot)
                total = send[target].astype(f32) + merge[slot].astype(f32)
                send[target] = total.astype(bf16)
                described(send.at[target], recv.at[1], "kv", target, sent, received).start()

        if merged:
            when(paired_inner, both)

    def sum_wait(started):
        send, recv, merge, merged, sent, received = started
        if merged:
            when(paired, lambda: arrived(recv.at[0:2], received))
            when(single, lambda: arrived(recv, received))
        else:
            arrived(recv, received)

    def spread_start(buffer, relayed, p, c):
        sent, received = spread_sems(p, c)
        relayed = relayed and line
        passed = parts * per_recv + p * len(bounds) + c

        def own(target, sem):
            described(buffer.at[kv], buffer.at[kv], "kv", target, sent, sem).start()

        def direct():
            for target in targets():
                own(target, received)

        def short():
            own(far_inner, passed)
            own(partner, received)

        if relayed:
            when(paired, short)
            when(single, direct)
            drain_later(paired_outer, buffer.at[0:2], sent)
            drain_later(paired_inner, buffer, sent)
            drain_later(single, buffer.at[0 : n_kv - 1], sent)
        else:
            direct()
            drain_later(None, buffer.at[0 : n_kv - 1], sent)
        return (buffer, relayed, sent, received, passed)

    def spread_pass(started):
        buffer, relayed, sent, received, passed = started

        def both():
            arrived(buffer.at[0:2], passed)
            for owner in (far_inner, far_outer):
                block = buffer.at[owner]
                described(block, block, "kv", partner, sent, passed).start()

        if relayed:
            when(paired_inner, both)

    def spread_wait(started):
        buffer, relayed, sent, received, passed = started
        if relayed:
            when(paired, lambda: arrived(buffer.at[0], received))
            when(paired_outer, lambda: arrived(buffer.at[0:2], passed))
            when(single, lambda: arrived(buffer.at[0 : n_kv - 1], received))
        else:
            arrived(buffer.at[0 : n_kv - 1], received)

    def gather_tp(buffer, p):
        sent, received = tp_sems(p)
        orders = []
        for me in range(2):
            keys = {o: (me + o in (1, n_tp), (me + o) % 2, o) for o in range(1, n_tp)}
            orders.append(sorted(keys, key=keys.get))
        for even, odd in zip(*orders):
            o = even + (odd - even) * lax.rem(tp, 2) if n_tp % 2 == 0 else even
            target = lax.rem(tp + o, n_tp)
            block = buffer.at[tp]
            described(block, block, "tp", target, sent, received + 2).start()
        drain_later(None, buffer.at[0 : n_tp - 1], sent)

    def gather_wait(buffer, p):
        arrived(buffer.at[0 : n_tp - 1], tp_sems(p)[1] + 2)

    def store_all(buffer, lo, value):
        for p in range(parts):
            for d in range(n_kv):
                first = d * seqs + p * sub
                buffer[p, d, :, lo : lo + value.shape[1]] = value[first : first + sub]

    def store_rows(buffer, p, lo, value):
        for d in range(n_kv):
            buffer[p, d, :, lo : lo + value.shape[1]] = value[d * sub : (d + 1) * sub]

    def rows_of(value, p):
        pieces = [value[d * seqs + p * sub : d * seqs + (p + 1) * sub] for d in range(n_kv)]
        return jnp.concatenate(pieces, axis=0)

    def joined(block):
        return block.astype(f32).reshape(rows, block.shape[2]).astype(bf16)

    def reduced(send, recv, p, lo, hi):
        total = send[p, kv, :, lo:hi].astype(f32)
        for o in range(n_kv - 1):
            total = total + recv[p, o, :, lo:hi].astype(f32)
        return total

    if line:

        @pl.when(paired)
        def _():
            for buffer, chosen in ((a_recv, MERGE_A), (b_recv, MERGE_B)):
                for p in chosen:
                    buffer[p, n_kv - 2] = jnp.zeros(buffer.shape[2:], bf16)
            for buffer in gu_recv:
                for p in MERGE_GU:
                    buffer[p, n_kv - 2] = jnp.zeros(buffer.shape[2:], bf16)

    copies["tokens"].wait()
    copies["g_mix"].wait()
    inputs = vm["tokens"][...].astype(f32)
    scaled = (inputs * gain("g_mix")).astype(bf16)
    store_all(a_send, 2 * kw, split_hi_lo(jnp.sum(inputs * inputs, axis=1, keepdims=True)))
    for name in ("w_query", "w_key", "w_decay"):
        copies[name].wait()
    for index, name in enumerate(("w_query", "w_decay")):
        part = jnp.dot(scaled, vm[name][...], preferred_element_type=f32)
        store_all(a_send, index * kw, part.astype(bf16))
    for name in names[EARLY:LAST]:
        copies[name].start()
    copies["lengths"].start()
    pl.semaphore_wait(barrier, n_kv - 1 + n_tp - 1)
    def start_a(p, who=None):
        return sum_start(a_send.at[p], a_recv.at[p], a_merge.at[p], p in MERGE_A, p, 0, who)

    def start_b(p, who=None):
        return sum_start(b_send.at[p], b_recv.at[p], b_merge.at[p], p in MERGE_B, p, 1, who)

    sent_a = [start_a(0)]
    for name in ("w_value", "w_outgate"):
        copies[name].wait()
    for index, name in enumerate(("w_value", "w_outgate")):
        part = jnp.dot(scaled, vm[name][...], preferred_element_type=f32)
        store_all(b_send, index * vw, part.astype(bf16))
    part = jnp.dot(scaled, vm["w_key"][...], preferred_element_type=f32)
    store_all(b_send, 2 * vw, part.astype(bf16))
    first = single if line and YIELD else None
    sent_b = [start_b(0, first if YIELD == 2 else None)]
    for p in range(1, parts):
        sent_a.append(start_a(p, first))
        sent_b.append(start_b(p, first))

    copies["cum_decay"].wait()
    copies["state"].wait()
    copies["lengths"].wait()
    ordinal = lax.broadcasted_iota(jnp.int32, (block_len, dk), 0)

    group = 8 if sub % 8 == 0 else sub

    def prepare(step, carry):
        base = pl.multiple_of(step * group, group)
        for h in range(heads):
            ends = []
            for inner in range(group):
                s = base + inner
                live = lax.rem(lengths[s], block_len)
                picked = jnp.where(ordinal == live - 1, vm["cum_decay"][s, h], 0.0)
                ends.append(jnp.sum(picked, axis=0, keepdims=True))
                state_bf[s, h] = vm["state"][s, h].astype(bf16)
            td_base[pl.ds(base, group), h * dk : (h + 1) * dk] = jnp.concatenate(ends, axis=0)
        return carry

    lax.fori_loop(0, seqs // group, prepare, 0)
    if line and YIELD:
        if YIELD == 2:
            start_b(0, paired)
        for p in range(1, parts):
            start_a(p, paired)
            start_b(p, paired)
    for name in ("step_decay", "key_block", "value_block", "g_heads"):
        copies[name].wait()
    for name in names[LAST:]:
        copies[name].start()

    live_ordinal = lax.broadcasted_iota(jnp.int32, (block_len, 1), 0)

    def attend(step, carry):
        base = pl.multiple_of(step * group, group)
        for h in range(heads):
            cols = slice(h * dk, (h + 1) * dk)
            qs = q_ref[pl.ds(base, group), cols]
            tds = td_ref[pl.ds(base, group), cols]
            qes = qe_ref[pl.ds(base, group), cols]
            outs = []
            for inner in range(group):
                s = base + inner
                live = lax.rem(lengths[s], block_len)
                left = jnp.broadcast_to(qes[inner : inner + 1], (16, dk)).astype(bf16)
                carried = jnp.dot(left, state_bf[s, h], preferred_element_type=f32)[:1]
                scores = jnp.sum(
                    qs[inner : inner + 1]
                    * vm["key_block"][s, h].astype(f32)
                    * jnp.exp(tds[inner : inner + 1] - vm["cum_decay"][s, h]),
                    axis=1,
                    keepdims=True,
                )
                scores = jnp.where(live_ordinal < live, scores, 0.0)
                in_block = jnp.sum(
                    scores * vm["value_block"][s, h].astype(f32), axis=0, keepdims=True
                )
                outs.append(carried + in_block)
            head_ref[pl.ds(base, group), h * dv : (h + 1) * dv] = jnp.concatenate(outs, axis=0)
        return carry

    sum_merge(sent_a[0])
    sum_merge(sent_b[0])
    sent_mixed = []
    for p in range(parts):
        own_rows = slice(p * sub, (p + 1) * sub)
        sum_wait(sent_a[p])
        square = join_hi_lo(reduced(a_send, a_recv, p, 2 * kw, 2 * kw + LANES))
        inverse = lax.rsqrt(square / width + epsilon)
        query = reduced(a_send, a_recv, p, 0, kw) * inverse * dk ** (-0.5)
        decay_pre = reduced(a_send, a_recv, p, kw, 2 * kw) * inverse
        log_sigmoid = jnp.minimum(decay_pre, 0.0) - jnp.log(1.0 + jnp.exp(-jnp.abs(decay_pre)))
        log_step = log_sigmoid / temper + vm["step_decay"][own_rows]
        token_decay = td_base[own_rows] + log_step
        q_ref[own_rows] = query
        td_ref[own_rows] = token_decay
        qe_ref[own_rows] = query * jnp.exp(token_decay)
        lax.fori_loop(p * sub // group, (p + 1) * sub // group, attend, 0)
        sum_wait(sent_b[p])
        keys_new = reduced(b_send, b_recv, p, 2 * vw, 2 * vw + kw) * inverse
        for h in range(heads):
            cols = slice(h * dv, (h + 1) * dv)
            keys = slice(h * dk, (h + 1) * dk)
            values_new = reduced(b_send, b_recv, p, h * dv, (h + 1) * dv) * inverse
            out_gate = reduced(b_send, b_recv, p, vw + h * dv, vw + (h + 1) * dv) * inverse
            own = jnp.sum(query[:, keys] * keys_new[:, keys], axis=1, keepdims=True)
            head_out = head_ref[own_rows, cols] + own * values_new
            scale = lax.rsqrt(jnp.mean(head_out * head_out, axis=1, keepdims=True) + epsilon)
            normed = head_out * scale * gain("g_heads")[:, cols]
            mixed_all[p, kv, :, cols] = (normed * silu(out_gate)).astype(bf16)
        sent_mixed.append(spread_start(mixed_all.at[p], False, p, 0))
        if p + 1 < parts:
            sum_merge(sent_a[p + 1])
            sum_merge(sent_b[p + 1])

    copies["w_out"].wait()
    by_chip = n_tp % 2 == 0
    chip = tp // 2
    chips = n_tp // 2
    mine = chips + lax.rem(tp, 2)
    other = chips + 1 - lax.rem(tp, 2)
    beside = tp + 1 - 2 * lax.rem(tp, 2)

    def chip_sum(p, condition):
        there, here = attn_all.at[p, mine], attn_all.at[p, chip]
        sent, received = tp_sems(p)

        def add():
            arrived(attn_all.at[p, other], received)
            both = attn_all[p, mine].astype(f32) + attn_all[p, other].astype(f32)
            attn_all[p, chip] = both.astype(bf16)
            for o in range(1, chips):
                target = lax.rem(tp + 2 * o, n_tp)
                described(here, here, "tp", target, sent, received + 1).start()

        when(condition, add)

    def chip_wait(p):
        if chips > 1:
            arrived(attn_all.at[p, 0 : chips - 1], tp_sems(p)[1] + 1)

    for p in range(parts):
        spread_wait(sent_mixed[p])
        part = jnp.dot(joined(mixed_all[p]), vm["w_out"][...], preferred_element_type=f32)
        attn_all[p, mine if by_chip else tp] = part.astype(bf16)
        if by_chip:
            there = attn_all.at[p, mine]
            sent, received = tp_sems(p)
            described(there, there, "tp", beside, sent, received).start()
            chip_sum(p, single)
        else:
            gather_tp(attn_all.at[p], p)
    if by_chip:
        for p in range(parts):
            chip_sum(p, paired)
    drain()

    copies["g_ffn"].wait()
    copies["w_gate"].wait()
    copies["w_up"].wait()
    middles = []
    sent_gu = []
    for p in range(parts):
        if by_chip:
            chip_wait(p)
            drain_later(None, attn_all.at[p, 0:chips], tp_sems(p)[0])
        else:
            gather_wait(attn_all.at[p], p)
        attention = attn_all[p, 0].astype(f32)
        for t in range(1, chips if by_chip else n_tp):
            attention = attention + attn_all[p, t].astype(f32)
        middle = (rows_of(inputs, p) + attention).astype(bf16).astype(f32)
        normed_mid = (middle * gain("g_ffn")).astype(bf16)
        middles.append(middle)
        sent_gu.append([])
        for c, (lo, hi) in enumerate(bounds):
            if c == 0:
                square = jnp.sum(middle * middle, axis=1, keepdims=True)
                store_rows(gu_send[c], p, 2 * (hi - lo), split_hi_lo(square))
            for index, name in enumerate(("w_gate", "w_up")):
                part = jnp.dot(normed_mid, vm[name][:, lo:hi], preferred_element_type=f32)
                store_rows(gu_send[c], p, index * (hi - lo), part.astype(bf16))
            refs = (gu_send[c].at[p], gu_recv[c].at[p], gu_merge[c].at[p])
            sent_gu[p].append(sum_start(*refs, p in MERGE_GU, p, c))
    gate_drains = len(drains)
    order = [(p, c) for p in range(parts) for c in range(len(bounds))]
    start = min(len(order), len(bounds) + AHEAD)
    ahead = order[start:]
    for p, c in order[:start]:
        sum_merge(sent_gu[p][c])
    sent_hid = [[] for _ in range(parts)]
    passing = []
    for p, c in order:
        lo, hi = bounds[c]
        w = hi - lo
        sum_wait(sent_gu[p][c])
        if c == 0:
            total = join_hi_lo(reduced(gu_send[c], gu_recv[c], p, 2 * w, 2 * w + LANES))
            mid_inverse = lax.rsqrt(total / width + epsilon)
        gate = reduced(gu_send[c], gu_recv[c], p, 0, w) * mid_inverse
        up = reduced(gu_send[c], gu_recv[c], p, w, 2 * w) * mid_inverse
        hid_all[c][p, kv] = (silu(gate) * up).astype(bf16)
        sent_hid[p].append(spread_start(hid_all[c].at[p], p in RELAY, p, c))
        passing.append(sent_hid[p][c])
        if ahead:
            q, e = ahead.pop(0)
            sum_merge(sent_gu[q][e])
        elif len(passing) > 1:
            spread_pass(passing.pop(0))
    copies["w_down"].wait()
    held = drains[:]
    drains.clear()
    for condition, copy in held[:gate_drains]:
        when(condition, copy.wait_send)
    for p in range(parts):
        if p == parts - 1:
            for started in passing:
                spread_pass(started)
        down = None
        for c, (lo, hi) in enumerate(bounds):
            spread_wait(sent_hid[p][c])
            part = jnp.dot(joined(hid_all[c][p]), vm["w_down"][lo:hi], preferred_element_type=f32)
            down = part if down is None else down + part
        down_all[p, tp] = down.astype(bf16)
        gather_tp(down_all.at[p], p)
    for condition, copy in held[gate_drains:]:
        when(condition, copy.wait_send)
    finals = []
    for p in range(parts):
        gather_wait(down_all.at[p], p)
        total = down_all[p, 0].astype(f32)
        for t in range(1, n_tp):
            total = total + down_all[p, t].astype(f32)
        finals.append(middles[p] + total)
    ordered = [finals[p][d * sub : (d + 1) * sub] for d in range(n_kv) for p in range(parts)]
    out_ref[...] = jnp.concatenate(ordered, axis=0).astype(bf16)
    drain()


ORDER = (
    "tokens",
    "g_mix",
    "w_query",
    "w_key",
    "w_decay",
    "w_value",
    "w_outgate",
    "cum_decay",
    "state",
    "step_decay",
    "key_block",
    "value_block",
    "g_heads",
    "w_out",
    "g_ffn",
    "w_gate",
    "w_up",
    "w_down",
)
SHARES = (3, 5, 3)
AHEAD = 1
PARTS = 2
YIELD = 0
FAR = True
RELAY = (0,)
MERGE_A = (1,)
MERGE_B = (1,)
MERGE_GU = (0, 1)
EARLY = 7
FIRST = 5
LAST = 13


def body(n_kv, n_tp, lengths, given):
    rows, columns = given["tokens"].shape
    seqs, heads, dk, dv = given["state"].shape
    kw, vw = heads * dk, heads * dv
    hidden = given["w_gate"].shape[1]
    tiles = -(-hidden // LANES)
    ends = [sum(SHARES[:c]) for c in range(len(SHARES) + 1)]
    edges = sorted({min(-(-tiles * end // ends[-1]) * LANES, hidden) for end in ends})
    chunks = len(edges) - 1
    bounds = tuple(zip(edges[:-1], edges[1:]))
    widths = [hi - lo for lo, hi in bounds]
    gu_widths = [2 * w + (LANES if c == 0 else 0) for c, w in enumerate(widths)]
    out_cols = given["w_out"].shape[1]
    parts = PARTS if seqs % (8 * PARTS) == 0 else 1
    sub = seqs // parts
    scratch = [pltpu.SMEM(lengths.shape, lengths.dtype)]
    scratch += [pltpu.VMEM(given[name].shape, given[name].dtype) for name in ORDER]
    scratch += [
        pltpu.VMEM((seqs, kw), f32),
        pltpu.VMEM((seqs, heads, dk, dv), bf16),
        pltpu.VMEM((seqs, kw), f32),
        pltpu.VMEM((seqs, kw), f32),
        pltpu.VMEM((seqs, kw), f32),
        pltpu.VMEM((seqs, vw), f32),
        pltpu.VMEM((parts, n_kv, sub, 2 * kw + LANES), bf16),
        pltpu.VMEM((parts, n_kv - 1, sub, 2 * kw + LANES), bf16),
        pltpu.VMEM((parts, n_kv, sub, 2 * vw + kw), bf16),
        pltpu.VMEM((parts, n_kv - 1, sub, 2 * vw + kw), bf16),
        pltpu.VMEM((parts, 2, sub, 2 * kw + LANES), bf16),
        pltpu.VMEM((parts, 2, sub, 2 * vw + kw), bf16),
        pltpu.VMEM((parts, n_kv, sub, vw), bf16),
        pltpu.VMEM((parts, max(n_tp, n_tp // 2 + 2), n_kv * sub, out_cols), bf16),
        [pltpu.VMEM((parts, n_kv, sub, w), bf16) for w in gu_widths],
        [pltpu.VMEM((parts, n_kv - 1, sub, w), bf16) for w in gu_widths],
        [pltpu.VMEM((parts, 2, sub, w), bf16) for w in gu_widths],
        [pltpu.VMEM((parts, n_kv, sub, w), bf16) for w in widths],
        pltpu.VMEM((parts, n_tp, n_kv * sub, out_cols), bf16),
        pltpu.SemaphoreType.DMA((LAST + 1 - FIRST,)),
        pltpu.SemaphoreType.DMA((parts * (max(2, chunks) + chunks + 1),)),
        pltpu.SemaphoreType.DMA((parts * (3 * max(2, chunks) + chunks + 3) + len(RELAY) * chunks,)),
    ]
    cfg = (n_kv, n_tp, ORDER, bounds, parts)
    return pl.pallas_call(
        functools.partial(kernel, cfg),
        out_shape=pltpu.VMEM((rows, columns), bf16),
        in_specs=[pl.BlockSpec(memory_space=pltpu.HBM)] * (len(ORDER) + 1),
        out_specs=pl.BlockSpec(memory_space=pltpu.VMEM),
        scratch_shapes=scratch,
        compiler_params=pltpu.CompilerParams(collective_id=0, has_side_effects=True),
        name="layer",
    )(*[given[name] for name in ORDER], lengths)


NAMES = (
    "tokens",
    "lengths",
    "state",
    "key_block",
    "value_block",
    "cum_decay",
    "step_decay",
    "g_mix",
    "w_query",
    "w_key",
    "w_value",
    "w_outgate",
    "w_decay",
    "g_heads",
    "w_out",
    "g_ffn",
    "w_gate",
    "w_up",
    "w_down",
)


def solution(mesh):
    def call(*arrays):
        given = dict(zip(NAMES, arrays))
        lengths = given.pop("lengths")
        return body(mesh.shape["kv"], mesh.shape["tp"], lengths, given)

    return jax.shard_map(
        call,
        mesh=mesh,
        in_specs=(
            P("grp", "kv"),
            P(("grp", "kv")),
            P(("grp", "kv"), "tp", None, None),
            P(("grp", "kv"), "tp", None, None),
            P(("grp", "kv"), "tp", None, None),
            P(("grp", "kv"), "tp", None, None),
            P(("grp", "kv"), "tp"),
            P("kv"),
            P("kv", "tp"),
            P("kv", "tp"),
            P("kv", "tp"),
            P("kv", "tp"),
            P("kv", "tp"),
            P("tp"),
            P("tp", "kv"),
            P("kv"),
            P("kv", "tp"),
            P("kv", "tp"),
            P("tp", "kv"),
        ),
        out_specs=P("grp", "kv"),
        check_vma=False,
    )
```
